32 devices in a mesh: fs: 8 (over z, x), tp: 4 (over y, core).
Axes of the slice: x: 2, y: 2, z: 4, core: 2. Of those that a mesh axis runs over, the one named last changes fastest.
Arguments:
- tokens: bfloat16 [4096, 2048], P(('fs', 'tp')), may hold values from -6 to 6
- norm_gain: float32 [2048], replicated, may hold values from 0.1 to 1.9
- up_weight: bfloat16 [2048, 8192], P('fs', 'tp'), may hold values from -0.125 to 0.125
- down_weight: bfloat16 [8192, 2048], P('tp', 'fs'), may hold values from -0.0625 to 0.0625
Outputs:
- mixed: bfloat16 [4096, 2048], P(('fs', 'tp'))
The draws below stay inside these ranges and needn't reach their ends.
All inputs are finite; a program needn't handle non-finite values.
Results may differ from the reference program's by a relative error of at most 0.013.
Values may be sent and summed in bfloat16 or wider, within the bound.
A program may use at most 64 MiB of HBM per device.

```python
import jax
import jax.numpy as jnp
from jax import lax

D = 2048
FF = 8192
TOKENS = 4096
N_TP = 4


def level_of(own_key, extent, shards, low, largest):
    loudness, own = 1.0, jax.random.fold_in(own_key, 6)
    for axis_at, parts in shards:
        heights = jnp.exp(jax.random.uniform(jax.random.fold_in(own, axis_at), (parts,), jnp.float32, low / len(shards), largest / len(shards)))
        loudness = loudness * jnp.repeat(heights, extent[axis_at] // parts).reshape([-1 if axis == axis_at else 1 for axis in range(len(extent))])
    return loudness


def normal_values(own_key, extent, deviation, reach, split=(), held_as=jnp.bfloat16):
    array = jax.random.normal(own_key, extent, jnp.float32) * deviation
    if len(split) > 0:
        array = level_of(own_key, extent, split, -0.22, 0.18) * array
    return jnp.clip(array, min=-reach, max=reach).astype(held_as)


def setup_inputs(seed: int = 0) -> dict:
    streams_of = jax.random.split(jax.random.key(seed), 5)
    return {
        "tokens": normal_values(streams_of[0], (TOKENS, D), 1.0, 6.0, ((0, 32),)),
        "norm_gain": jnp.clip(1.0 + 0.18 * jax.random.normal(streams_of[1], (D,), jnp.float32), 0.1, 1.9),
        "up_weight": normal_values(streams_of[2], (D, FF), D ** -0.5, 0.125, ((0, 8), (1, 4))),
        "down_weight": normal_values(streams_of[3], (FF, D), FF ** -0.5, 0.0625, ((0, 4), (1, 8))),
    }


epsilon = 1e-06

def reference(tokens, norm_gain, up_weight, down_weight):
    values = tokens.astype(jnp.float32)
    mean_square = lax.optimization_barrier(jnp.mean(values * values, axis=-1, keepdims=True))
    normed = (values * lax.rsqrt(mean_square + epsilon) * norm_gain).astype(jnp.bfloat16)
    preact = jnp.dot(normed, up_weight, preferred_element_type=jnp.float32)
    hidden = jnp.square(jnp.maximum(preact, 0.0)).astype(jnp.bfloat16)
    width = FF // N_TP
    total = jnp.zeros((tokens.shape[0], D), jnp.float32)
    for block in range(N_TP):
        columns = hidden[:, block * width:(block + 1) * width]
        rows_down = down_weight[block * width:(block + 1) * width, :]
        partial_value = jnp.dot(columns, rows_down, preferred_element_type=jnp.float32).astype(jnp.bfloat16)
        partial_value = lax.optimization_barrier(partial_value)
        total = total + partial_value.astype(jnp.float32)
    return total.astype(jnp.bfloat16)
```

```python
import functools
import math

import jax
import jax.numpy as jnp
from jax import lax
from jax.experimental import pallas as pl
from jax.experimental.pallas import tpu as pltpu
from jax.sharding import PartitionSpec as P

epsilon = 1e-06
MESH = pl.DeviceIdType.MESH
f32, bf16 = jnp.float32, jnp.bfloat16


def plain(tokens, norm_gain, up_weight, down_weight):
    values = tokens.astype(f32)
    mean_square = jnp.mean(values * values, axis=-1, keepdims=True)
    normed = (values * lax.rsqrt(mean_square + epsilon) * norm_gain).astype(bf16)
    up_whole = lax.all_gather(up_weight, "fs", axis=0, tiled=True)
    rows = lax.all_gather(normed, "tp", axis=0, tiled=True)
    preact = jnp.dot(rows, up_whole, preferred_element_type=f32)
    hidden = jnp.square(jnp.maximum(preact, 0.0)).astype(bf16)
    down_whole = lax.all_gather(down_weight, "fs", axis=1, tiled=True)
    partial_value = jnp.dot(hidden, down_whole, preferred_element_type=f32).astype(bf16)
    return lax.psum_scatter(partial_value, "tp", scatter_dimension=0, tiled=True)


PROGRAM = {
    0: [
        ("uown",), ("usend", 1), ("usend", 2), ("usend", 3), ("tsend",),
        ("urel", 1), ("udiag", 0), ("urel", 2), ("udiag", 1), ("urel", 3), ("udiag", 2),
        ("dsend", 1), ("udiag", 3), ("down_own",), ("trel", 1, 0), ("trel", 1, 1),
        ("trel", 2, 0), ("dsend", 2), ("dsend", 3), ("trel", 2, 1),
        ("uall", 0), ("uall", 1), ("uall", 2), ("uall", 3),
        ("hid", 0), ("hid", 1), ("drel", 1), ("ddiag", 0), ("hid", 2), ("ddiag", 1),
        ("trel", 3, 0), ("trel", 3, 1), ("dall", 0), ("hid", 3),
        ("proj", 0, (3, 2, 1, 0)), ("sum", 3, 0), ("sum", 2, 0), ("sum", 1, 0),
        ("dall", 1), ("proj", 1, (3, 2, 1, 0)), ("sum", 3, 1), ("sum", 2, 1), ("sum", 1, 1),
        ("drel", 2), ("ddiag", 2), ("drel", 3), ("ddiag", 3),
        ("dall", 2), ("proj", 2, (3, 2, 1, 0)), ("sum", 3, 2), ("sum", 2, 2), ("sum", 1, 2),
        ("dall", 3), ("proj", 3, (3, 2, 1, 0)), ("sum", 3, 3), ("sum", 2, 3), ("sum", 1, 3),
        ("sum", 0, 3), ("sum", 0, 2), ("sum", 0, 1), ("sum", 0, 0),
    ],
    1: [
        ("uown",), ("usend", 2), ("usend", 3), ("usend", 0), ("tsend",), ("dsend", 0),
        ("urel", 0), ("urel", 2), ("udiag", 1), ("udiag", 0), ("udiag", 2), ("urel", 3),
        ("udiag", 3), ("down_own",),
        ("trel", 0, 0), ("trel", 2, 0), ("trel", 0, 1), ("trel", 2, 1), ("dsend", 2), ("dsend", 3),
        ("uall", 0), ("uall", 1), ("uall", 2), ("uall", 3),
        ("hid", 1), ("ddiag", 1), ("hid", 0), ("trel", 3, 0), ("hid", 2), ("trel", 3, 1),
        ("drel", 0), ("ddiag", 0), ("hid", 3), ("dall", 1), ("proj", 1, (0, 1, 2, 3)),
        ("dall", 0), ("proj", 0, (3, 2, 1, 0)), ("sum", 3, 0), ("sum", 2, 0),
        ("drel", 3), ("ddiag", 3), ("drel", 2), ("ddiag", 2),
        ("dall", 3), ("proj", 3, (0, 1, 2, 3)), ("sum", 0, 3), ("sum", 3, 1), ("sum", 2, 1),
        ("dall", 2), ("proj", 2, (0, 1, 2, 3)), ("sum", 0, 2),
        ("sum", 3, 2), ("sum", 2, 2), ("sum", 0, 1), ("sum", 3, 3), ("sum", 2, 3), ("sum", 0, 0),
        ("sum", 1, 0), ("sum", 1, 1), ("sum", 1, 2), ("sum", 1, 3),
    ],
}


def kernel(Z, X, Y, C, tok, gain, up, down, out,
           tokb, upb, downb, tokg, upg, downg, hid, part, cin, zin, zout, outb,
           in_s, out_s, wz_s, wz_r, wx_s, wx_r, wy_s, wy_r, wd_s, wd_r,
           t_s, t_r, tc_s, tc_r, rc_s, rc_r, rz_s, rz_r):
    T, D = tok.shape
    F = Z * X
    Dl = up.shape[0]
    B = upg.shape[2]
    fs, tp = lax.axis_index("fs"), lax.axis_index("tp")
    z, x = fs // X, fs % X
    y, c = tp // C, tp % C
    ox, oy, oc = X - 1 - x, Y - 1 - y, C - 1 - c
    low = z < Z // 2
    p = jnp.where(low, z, Z - 1 - z)
    side = jnp.where(low, 0, 1)

    def plane(q):
        return jnp.where(low, q, Z - 1 - q)

    def dev(zz=z, xx=x, yy=y, cc=c):
        return {"fs": zz * X + xx, "tp": yy * C + cc}

    def rcopy(src, dst, ss, rs, device):
        return pltpu.make_async_remote_copy(
            src_ref=src, dst_ref=dst, send_sem=ss, recv_sem=rs,
            device_id=device, device_id_type=MESH)

    def rows(start, size):
        return pl.ds(pl.multiple_of(start, size), size)

    barrier = pltpu.get_barrier_semaphore()
    peers = [dev(zz=(z + k) % Z) for k in range(1, Z)]
    peers += [dev(xx=ox), dev(yy=oy), dev(cc=oc)]
    for peer in peers:
        pl.semaphore_signal(barrier, inc=1, device_id=peer, device_id_type=MESH)

    loads = [
        pltpu.make_async_copy(tok, tokb, in_s.at[0]),
        pltpu.make_async_copy(up, upb, in_s.at[1]),
        pltpu.make_async_copy(down, downb, in_s.at[2]),
        pltpu.make_async_copy(up.at[:, rows(z * B, B)], upg.at[y, rows(fs * Dl, Dl)], in_s.at[3]),
        pltpu.make_async_copy(down.at[rows(z * B, B)], downg.at[fs, rows(y * B, B)], in_s.at[4]),
    ]
    for load in loads:
        load.start()
    loads[0].wait()
    RB = 32

    @pl.loop(0, T // RB)
    def _(i):
        v = tokb[rows(i * RB, RB), :].astype(f32)
        ms = jnp.mean(v * v, axis=-1, keepdims=True)
        tokg[z, rows(c * T + i * RB, RB), :] = (v * lax.rsqrt(ms + epsilon) * gain[...]).astype(bf16)

    for load in loads[1:]:
        load.wait()
    pl.semaphore_wait(barrier, len(peers))

    def piece(zz, xx, yy, k, half=None):
        f = zz * X + xx
        if k == 0:
            r = rows(f * Dl, Dl) if half is None else rows(f * Dl + half * (Dl // 2), Dl // 2)
            return upg.at[yy, r]
        r = rows(yy * B, B) if half is None else rows(yy * B + half * (B // 2), B // 2)
        return downg.at[f, r]

    def own_piece(zz, k):
        return upb.at[:, rows(zz * B, B)] if k == 0 else downb.at[rows(zz * B, B)]

    def wz(q, k):
        zz = plane(q)
        return rcopy(own_piece(zz, k), piece(z, x, y, k), wz_s.at[k, zz], wz_r.at[k, z], dev(zz=zz))

    def wz_recv(q, k):
        zz = plane(q)
        ref = piece(zz, x, y, k)
        return rcopy(ref, ref, wz_s.at[k, zz], wz_r.at[k, zz], dev(zz=zz))

    def wx(q, k, xx=x):
        zz = plane(q)
        ref = piece(zz, xx, y, k)
        return rcopy(ref, ref, wx_s.at[k, zz], wx_r.at[k, zz], dev(xx=ox))

    def wy(q, k, yy=y):
        zz = plane(q)
        ref = piece(zz, x, yy, k)
        return rcopy(ref, ref, wy_s.at[k, zz], wy_r.at[k, zz], dev(yy=oy))

    def wd(q, k, half):
        zz = plane(q)
        ref = piece(zz, ox, y, k, 0) if half == 0 else piece(zz, x, oy, k, 1)
        to = dev(yy=oy) if half == 0 else dev(xx=ox)
        return rcopy(ref, ref, wd_s.at[k, zz, half], wd_r.at[k, zz, half], to)

    def wd_recv(q, k, half):
        zz = plane(q)
        ref = piece(zz, ox, oy, k, half)
        return rcopy(ref, ref, wd_s.at[k, zz, half], wd_r.at[k, zz, half], dev(yy=oy))

    TH = T // 2

    def tok_z(g, half, way):
        gg = plane(g)
        ref = tokg.at[gg, rows(c * T + half * TH, TH)]
        to = jnp.where(low, z + way, z - way)
        return rcopy(ref, ref, t_s.at[(way + 1) // 2, gg, half], t_r.at[gg, half], dev(zz=to))

    def tok_c(g, half, cc=c):
        gg = plane(g)
        ref = tokg.at[gg, rows(cc * T + half * TH, TH)]
        return rcopy(ref, ref, tc_s.at[gg, half], tc_r.at[gg, half], dev(cc=oc))

    NB = min(B, 256)

    def compute(g):
        gg = plane(g)
        for yy in range(Y):
            @pl.loop(0, B // NB)
            def _(j):
                h = jnp.dot(tokg[gg], upg[yy, :, rows(j * NB, NB)], preferred_element_type=f32)
                h = jnp.maximum(h, 0.0)
                hid[gg, :, rows(yy * B + j * NB, NB)] = (h * h).astype(bf16)

    def sum_c(gg, f):
        return rcopy(part.at[gg, f, oc], cin.at[gg, f], rc_s.at[gg, f], rc_r.at[gg, f], dev(cc=oc))

    def project(q, gs):
        for g in gs:
            gg = plane(g)

            @pl.loop(0, X)
            def _(xx):
                f = plane(q) * X + xx
                v = jnp.dot(hid[gg], downg[f], preferred_element_type=f32).astype(bf16)
                for cc in range(C):
                    part[gg, f, cc] = v[cc * T:(cc + 1) * T]
                sum_c(gg, f).start()

    def sum_z(gg, f, way):
        to = jnp.where(low, z + way, z - way)
        at = side if way > 0 else 1 - side
        return rcopy(zout.at[gg, f], zin.at[at, gg, f], rz_s.at[gg, f], rz_r.at[at, gg, f], dev(zz=to))

    def out_copy(f):
        cols = rows(f * Dl, Dl)
        return pltpu.make_async_copy(outb.at[:, cols], out.at[:, cols], out_s.at[f])

    def step(me, g, q):
        gg = plane(g)

        @pl.loop(0, X)
        def _(xx):
            f = plane(q) * X + xx
            sum_c(gg, f).wait_recv()
            acc = part[gg, f, c].astype(f32) + cin[gg, f].astype(f32)
            if me > 0 and g >= me:
                sum_z(gg, f, 1).wait_recv()
                acc = acc + zin[side, gg, f].astype(f32)
            if g <= me:
                sum_z(gg, f, -1).wait_recv()
                acc = acc + zin[1 - side, gg, f].astype(f32)
            if g == me:
                outb[:, rows(f * Dl, Dl)] = acc.astype(bf16)
                out_copy(f).start()
            else:
                zout[gg, f] = acc.astype(bf16)
                sum_z(gg, f, 1 if g > me else -1).start()

    def run(me, op, *args):
        if op == "uown" or op == "down_own":
            k = 0 if op == "uown" else 1
            wx(me, k).start()
            wy(me, k).start()
        elif op == "usend" or op == "dsend":
            wz(args[0], 0 if op == "usend" else 1).start()
        elif op == "urel" or op == "drel":
            k = 0 if op == "urel" else 1
            wz_recv(args[0], k).wait_recv()
            wx(args[0], k).start()
            wy(args[0], k).start()
        elif op == "udiag" or op == "ddiag":
            k = 0 if op == "udiag" else 1
            wx(args[0], k, ox).wait_recv()
            wd(args[0], k, 0).start()
            wy(args[0], k, oy).wait_recv()
            wd(args[0], k, 1).start()
        elif op == "uall" or op == "dall":
            k = 0 if op == "uall" else 1
            for half in range(2):
                wd_recv(args[0], k, half).wait_recv()
        elif op == "tsend":
            for half in range(2):
                tok_z(me, half, 1).start()
                if me > 0:
                    tok_z(me, half, -1).start()
            for half in range(2):
                tok_c(me, half).start()
        elif op == "trel":
            g, half = args
            tok_z(g, half, 1 if g < me else -1).wait_recv()
            if me > 0:
                tok_z(g, half, 1 if g < me else -1).start()
            tok_c(g, half).start()
        elif op == "hid":
            for half in range(2):
                tok_c(args[0], half, oc).wait_recv()
            compute(args[0])
        elif op == "proj":
            project(*args)
        elif op == "sum":
            step(me, *args)

    def drain(me):
        for q in range(Z):
            for k in range(2):
                if q != me:
                    wz(q, k).wait_send()
                wx(q, k).wait_send()
                wy(q, k).wait_send()
                for half in range(2):
                    wd(q, k, half).wait_send()
            for half in range(2):
                tok_c(q, half).wait_send()
                if q == me or me > 0:
                    if q <= me:
                        tok_z(q, half, 1).wait_send()
                    if q >= me and me > 0:
                        tok_z(q, half, -1).wait_send()

    for me in range(Z // 2):
        @pl.when(p == me)
        def _(me=me):
            for item in PROGRAM[me]:
                run(me, *item)
            drain(me)

    @pl.loop(0, F)
    def _(f):
        @pl.loop(0, Z)
        def _(gg):
            sum_c(gg, f).wait_send()

            @pl.when(gg != z)
            def _():
                sum_z(gg, f, 1).wait_send()
        out_copy(f).wait()


def solution(mesh):
    n_fs, n_tp = mesh.shape["fs"], mesh.shape["tp"]
    X = 2 ** (int(math.log2(n_fs)) // 2)
    Z = n_fs // X
    C = 2
    Y = n_tp // C
    placed = (P(("fs", "tp"), None), P(), P("fs", "tp"), P("tp", "fs"))

    def on_device(tokens, norm_gain, up_weight, down_weight):
        T, D = tokens.shape
        Dl, FFl = up_weight.shape
        B = FFl // Z
        if X != 2 or Y != 2 or Z != 4 or Z * X != n_fs or Dl % 256 or B % 256 or T % 32:
            return plain(tokens, norm_gain, up_weight, down_weight)
        F = Z * X
        dma = pltpu.SemaphoreType.DMA
        vm = pl.BlockSpec(memory_space=pltpu.VMEM)
        hbm = pl.BlockSpec(memory_space=pl.ANY)
        return pl.pallas_call(
            functools.partial(kernel, Z, X, Y, C),
            out_shape=jax.ShapeDtypeStruct((T, D), bf16),
            in_specs=[hbm, vm, hbm, hbm],
            out_specs=hbm,
            scratch_shapes=[
                pltpu.VMEM((T, D), bf16),
                pltpu.VMEM((Dl, FFl), bf16),
                pltpu.VMEM((FFl, Dl), bf16),
                pltpu.VMEM((Z, C * T, D), bf16),
                pltpu.VMEM((Y, D, B), bf16),
                pltpu.VMEM((F, Y * B, Dl), bf16),
                pltpu.VMEM((Z, C * T, Y * B), bf16),
                pltpu.VMEM((Z, F, C, T, Dl), bf16),
                pltpu.VMEM((Z, F, T, Dl), bf16),
                pltpu.VMEM((2, Z, F, T, Dl), bf16),
                pltpu.VMEM((Z, F, T, Dl), bf16),
                pltpu.VMEM((T, D), bf16),
                dma((5,)), dma((F,)),
                *[dma((2, Z)) for _ in range(6)],
                *[dma((2, Z, 2)) for _ in range(2)],
                dma((2, Z, 2)), dma((Z, 2)), dma((Z, 2)), dma((Z, 2)),
                dma((Z, F)), dma((Z, F)), dma((Z, F)), dma((2, Z, F)),
            ],
            compiler_params=pltpu.CompilerParams(
                collective_id=0, has_side_effects=True, vmem_limit_bytes=60 * 2**20),
        )(tokens, norm_gain.reshape(1, D), up_weight, down_weight)

    return jax.shard_map(
        on_device, mesh=mesh, in_specs=placed, out_specs=P(("fs", "tp"), None), check_vma=False)
```

```python
import functools
import math

import jax
import jax.numpy as jnp
from jax import lax
from jax.experimental import pallas as pl
from jax.experimental.pallas import tpu as pltpu
from jax.sharding import PartitionSpec as P

epsilon = 1e-06
MESH = pl.DeviceIdType.MESH
f32, bf16 = jnp.float32, jnp.bfloat16


def plain(tokens, norm_gain, up_weight, down_weight):
    values = tokens.astype(f32)
    mean_square = jnp.mean(values * values, axis=-1, keepdims=True)
    normed = (values * lax.rsqrt(mean_square + epsilon) * norm_gain).astype(bf16)
    up_whole = lax.all_gather(up_weight, "fs", axis=0, tiled=True)
    rows = lax.all_gather(normed, "tp", axis=0, tiled=True)
    preact = jnp.dot(rows, up_whole, preferred_element_type=f32)
    hidden = jnp.square(jnp.maximum(preact, 0.0)).astype(bf16)
    down_whole = lax.all_gather(down_weight, "fs", axis=1, tiled=True)
    partial_value = jnp.dot(hidden, down_whole, preferred_element_type=f32).astype(bf16)
    return lax.psum_scatter(partial_value, "tp", scatter_dimension=0, tiled=True)


PROGRAM = {
    0: [
        ("uown",), ("usend", 3), ("usend", 2), ("usend", 1), ("tsend",), ("dsend", 1),
        ("udiag", 0), ("urel", 3), ("urel", 1), ("udiag", 3), ("udiag", 1), ("urel", 2), ("udiag", 2),
        ("down_own",), ("drel", 1), ("trel", 1, 0), ("trel", 1, 1),
        ("uall", 0), ("uall", 1), ("uall", 2), ("uall", 3), ("hid", 0), ("hid", 1),
        ("dsend", 3), ("dsend", 2), ("ddiag", 0), ("trel", 2, 0), ("dall", 0),
        ("proj", 0, (1, 0)), ("sum", 1, 0), ("ddiag", 1), ("trel", 2, 1), ("drel", 3), ("hid", 2),
        ("proj", 0, (2,)), ("sum", 2, 0), ("dall", 1), ("proj", 1, (2, 1, 0)), ("sum", 2, 1), ("sum", 1, 1),
        ("trel", 3, 0), ("ddiag", 3), ("dall", 3), ("proj", 3, (2, 1, 0)), ("sum", 2, 3), ("sum", 1, 3),
        ("trel", 3, 1), ("drel", 2), ("hid", 3),
        ("proj", 0, (3,)), ("sum", 3, 0), ("proj", 1, (3,)), ("sum", 3, 1), ("proj", 3, (3,)), ("sum", 3, 3),
        ("ddiag", 2), ("dall", 2), ("proj", 2, (3, 2, 1, 0)), ("sum", 3, 2), ("sum", 2, 2), ("sum", 1, 2),
        ("sum", 0, 3), ("sum", 0, 2), ("sum", 0, 0), ("sum", 0, 1),
    ],
    1: [
        ("uown",), ("usend", 2), ("usend", 3), ("usend", 0), ("tsend",), ("dsend", 0),
        ("udiag", 1), ("urel", 3), ("urel", 0), ("urel", 2), ("udiag", 3), ("trel", 0, 0), ("udiag", 0),
        ("trel", 0, 1), ("trel", 2, 0), ("udiag", 2), ("down_own",), ("trel", 2, 1),
        ("dsend", 2), ("dsend", 3), ("drel", 0),
        ("uall", 0), ("uall", 1), ("uall", 2), ("uall", 3),
        ("hid", 1), ("hid", 0), ("trel", 3, 0), ("ddiag", 1), ("hid", 2), ("dall", 1), ("proj", 1, (2, 0, 1)),
        ("ddiag", 0), ("drel", 3), ("dall", 0), ("trel", 3, 1), ("proj", 0, (2, 0, 1)), ("sum", 2, 0),
        ("drel", 2), ("hid", 3), ("proj", 1, (3,)), ("proj", 0, (3,)), ("sum", 2, 1), ("ddiag", 3),
        ("dall", 3), ("proj", 3, (2, 3, 0, 1)), ("sum", 2, 3), ("ddiag", 2), ("sum", 3, 0), ("sum", 0, 3),
        ("sum", 3, 1), ("sum", 3, 3), ("sum", 0, 0),
        ("dall", 2), ("proj", 2, (0, 3, 2, 1)), ("sum", 0, 2), ("sum", 3, 2), ("sum", 2, 2), ("sum", 0, 1),
        ("sum", 1, 0), ("sum", 1, 3), ("sum", 1, 1), ("sum", 1, 2),
    ],
}


def kernel(Z, X, Y, C, tok, gain, up, down, out,
           tokb, upb, downb, tokg, upg, downg, hid, part, cin, zin, zout, outb,
           in_s, out_s, wz_s, wz_r, wx_s, wx_r, wy_s, wy_r, wd_s, wd_r,
           t_s, t_r, tc_s, tc_r, rc_s, rc_r, rz_s, rz_r):
    T, D = tok.shape
    F = Z * X
    Dl = up.shape[0]
    B = upg.shape[2]
    fs, tp = lax.axis_index("fs"), lax.axis_index("tp")
    z, x = fs // X, fs % X
    y, c = tp // C, tp % C
    ox, oy, oc = X - 1 - x, Y - 1 - y, C - 1 - c
    low = z < Z // 2
    p = jnp.where(low, z, Z - 1 - z)
    side = jnp.where(low, 0, 1)

    def plane(q):
        return jnp.where(low, q, Z - 1 - q)

    def dev(zz=z, xx=x, yy=y, cc=c):
        return {"fs": zz * X + xx, "tp": yy * C + cc}

    def rcopy(src, dst, ss, rs, device):
        return pltpu.make_async_remote_copy(
            src_ref=src, dst_ref=dst, send_sem=ss, recv_sem=rs,
            device_id=device, device_id_type=MESH)

    def rows(start, size):
        return pl.ds(pl.multiple_of(start, size), size)

    barrier = pltpu.get_barrier_semaphore()
    peers = [dev(zz=(z + k) % Z) for k in range(1, Z)]
    peers += [dev(xx=ox), dev(yy=oy), dev(cc=oc)]
    for peer in peers:
        pl.semaphore_signal(barrier, inc=1, device_id=peer, device_id_type=MESH)

    loads = [
        pltpu.make_async_copy(tok, tokb, in_s.at[0]),
        pltpu.make_async_copy(up, upb, in_s.at[1]),
        pltpu.make_async_copy(down, downb, in_s.at[2]),
        pltpu.make_async_copy(up.at[:, rows(z * B, B)], upg.at[y, rows(fs * Dl, Dl)], in_s.at[3]),
        pltpu.make_async_copy(down.at[rows(z * B, B)], downg.at[fs, rows(y * B, B)], in_s.at[4]),
    ]
    for load in loads:
        load.start()
    loads[0].wait()
    RB = 32

    @pl.loop(0, T // RB)
    def _(i):
        v = tokb[rows(i * RB, RB), :].astype(f32)
        ms = jnp.mean(v * v, axis=-1, keepdims=True)
        tokg[z, rows(c * T + i * RB, RB), :] = (v * lax.rsqrt(ms + epsilon) * gain[...]).astype(bf16)

    for load in loads[1:]:
        load.wait()
    pl.semaphore_wait(barrier, len(peers))

    def piece(zz, xx, yy, k, half=None):
        f = zz * X + xx
        if k == 0:
            r = rows(f * Dl, Dl) if half is None else rows(f * Dl + half * (Dl // 2), Dl // 2)
            return upg.at[yy, r]
        r = rows(yy * B, B) if half is None else rows(yy * B + half * (B // 2), B // 2)
        return downg.at[f, r]

    def own_piece(zz, k):
        return upb.at[:, rows(zz * B, B)] if k == 0 else downb.at[rows(zz * B, B)]

    def wz(q, k):
        zz = plane(q)
        return rcopy(own_piece(zz, k), piece(z, x, y, k), wz_s.at[k, zz], wz_r.at[k, z], dev(zz=zz))

    def wz_recv(q, k):
        zz = plane(q)
        ref = piece(zz, x, y, k)
        return rcopy(ref, ref, wz_s.at[k, zz], wz_r.at[k, zz], dev(zz=zz))

    def wx(q, k, xx=x):
        zz = plane(q)
        ref = piece(zz, xx, y, k)
        return rcopy(ref, ref, wx_s.at[k, zz], wx_r.at[k, zz], dev(xx=ox))

    def wy(q, k, yy=y):
        zz = plane(q)
        ref = piece(zz, x, yy, k)
        return rcopy(ref, ref, wy_s.at[k, zz], wy_r.at[k, zz], dev(yy=oy))

    def wd(q, k, half):
        zz = plane(q)
        ref = piece(zz, ox, y, k, 0) if half == 0 else piece(zz, x, oy, k, 1)
        to = dev(yy=oy) if half == 0 else dev(xx=ox)
        return rcopy(ref, ref, wd_s.at[k, zz, half], wd_r.at[k, zz, half], to)

    def wd_recv(q, k, half):
        zz = plane(q)
        ref = piece(zz, ox, oy, k, half)
        return rcopy(ref, ref, wd_s.at[k, zz, half], wd_r.at[k, zz, half], dev(yy=oy))

    TH = T // 2

    def tok_z(g, half, way):
        gg = plane(g)
        ref = tokg.at[gg, rows(c * T + half * TH, TH)]
        to = jnp.where(low, z + way, z - way)
        return rcopy(ref, ref, t_s.at[(way + 1) // 2, gg, half], t_r.at[gg, half], dev(zz=to))

    def tok_c(g, half, cc=c):
        gg = plane(g)
        ref = tokg.at[gg, rows(cc * T + half * TH, TH)]
        return rcopy(ref, ref, tc_s.at[gg, half], tc_r.at[gg, half], dev(cc=oc))

    NB = min(B, 256)

    def compute(g):
        gg = plane(g)
        for yy in range(Y):
            @pl.loop(0, B // NB)
            def _(j):
                h = jnp.dot(tokg[gg], upg[yy, :, rows(j * NB, NB)], preferred_element_type=f32)
                h = jnp.maximum(h, 0.0)
                hid[gg, :, rows(yy * B + j * NB, NB)] = (h * h).astype(bf16)

    def sum_c(gg, f):
        return rcopy(part.at[gg, f, oc], cin.at[gg, f], rc_s.at[gg, f], rc_r.at[gg, f], dev(cc=oc))

    def project(q, gs):
        for g in gs:
            gg = plane(g)

            @pl.loop(0, X)
            def _(xx):
                f = plane(q) * X + xx
                v = jnp.dot(hid[gg], downg[f], preferred_element_type=f32).astype(bf16)
                for cc in range(C):
                    part[gg, f, cc] = v[cc * T:(cc + 1) * T]
                sum_c(gg, f).start()

    def sum_z(gg, f, way):
        to = jnp.where(low, z + way, z - way)
        at = side if way > 0 else 1 - side
        return rcopy(zout.at[gg, f], zin.at[at, gg, f], rz_s.at[gg, f], rz_r.at[at, gg, f], dev(zz=to))

    def out_copy(f):
        cols = rows(f * Dl, Dl)
        return pltpu.make_async_copy(outb.at[:, cols], out.at[:, cols], out_s.at[f])

    def step(me, g, q):
        gg = plane(g)

        @pl.loop(0, X)
        def _(xx):
            f = plane(q) * X + xx
            sum_c(gg, f).wait_recv()
            acc = part[gg, f, c].astype(f32) + cin[gg, f].astype(f32)
            if me > 0 and g >= me:
                sum_z(gg, f, 1).wait_recv()
                acc = acc + zin[side, gg, f].astype(f32)
            if g <= me:
                sum_z(gg, f, -1).wait_recv()
                acc = acc + zin[1 - side, gg, f].astype(f32)
            if g == me:
                outb[:, rows(f * Dl, Dl)] = acc.astype(bf16)
                out_copy(f).start()
            else:
                zout[gg, f] = acc.astype(bf16)
                sum_z(gg, f, 1 if g > me else -1).start()

    def run(me, op, *args):
        if op == "uown" or op == "down_own":
            k = 0 if op == "uown" else 1
            wx(me, k).start()
            wy(me, k).start()
        elif op == "usend" or op == "dsend":
            wz(args[0], 0 if op == "usend" else 1).start()
        elif op == "urel" or op == "drel":
            k = 0 if op == "urel" else 1
            wz_recv(args[0], k).wait_recv()
            wx(args[0], k).start()
            wy(args[0], k).start()
        elif op == "udiag" or op == "ddiag":
            k = 0 if op == "udiag" else 1
            wx(args[0], k, ox).wait_recv()
            wd(args[0], k, 0).start()
            wy(args[0], k, oy).wait_recv()
            wd(args[0], k, 1).start()
        elif op == "uall" or op == "dall":
            k = 0 if op == "uall" else 1
            for half in range(2):
                wd_recv(args[0], k, half).wait_recv()
        elif op == "tsend":
            for half in range(2):
                tok_z(me, half, 1).start()
                if me > 0:
                    tok_z(me, half, -1).start()
            for half in range(2):
                tok_c(me, half).start()
        elif op == "trel":
            g, half = args
            tok_z(g, half, 1 if g < me else -1).wait_recv()
            if me > 0:
                tok_z(g, half, 1 if g < me else -1).start()
            tok_c(g, half).start()
        elif op == "hid":
            for half in range(2):
                tok_c(args[0], half, oc).wait_recv()
            compute(args[0])
        elif op == "proj":
            project(*args)
        elif op == "sum":
            step(me, *args)

    def drain(me):
        for q in range(Z):
            for k in range(2):
                if q != me:
                    wz(q, k).wait_send()
                wx(q, k).wait_send()
                wy(q, k).wait_send()
                for half in range(2):
                    wd(q, k, half).wait_send()
            for half in range(2):
                tok_c(q, half).wait_send()
                if q == me or me > 0:
                    if q <= me:
                        tok_z(q, half, 1).wait_send()
                    if q >= me and me > 0:
                        tok_z(q, half, -1).wait_send()

    for me in range(Z // 2):
        @pl.when(p == me)
        def _(me=me):
            for item in PROGRAM[me]:
                run(me, *item)
            drain(me)

    @pl.loop(0, F)
    def _(f):
        @pl.loop(0, Z)
        def _(gg):
            sum_c(gg, f).wait_send()

            @pl.when(gg != z)
            def _():
                sum_z(gg, f, 1).wait_send()
        out_copy(f).wait()


def solution(mesh):
    n_fs, n_tp = mesh.shape["fs"], mesh.shape["tp"]
    X = 2 ** (int(math.log2(n_fs)) // 2)
    Z = n_fs // X
    C = 2
    Y = n_tp // C
    placed = (P(("fs", "tp"), None), P(), P("fs", "tp"), P("tp", "fs"))

    def on_device(tokens, norm_gain, up_weight, down_weight):
        T, D = tokens.shape
        Dl, FFl = up_weight.shape
        B = FFl // Z
        if X != 2 or Y != 2 or Z != 4 or Z * X != n_fs or Dl % 256 or B % 256 or T % 32:
            return plain(tokens, norm_gain, up_weight, down_weight)
        F = Z * X
        dma = pltpu.SemaphoreType.DMA
        vm = pl.BlockSpec(memory_space=pltpu.VMEM)
        hbm = pl.BlockSpec(memory_space=pl.ANY)
        return pl.pallas_call(
            functools.partial(kernel, Z, X, Y, C),
            out_shape=jax.ShapeDtypeStruct((T, D), bf16),
            in_specs=[hbm, vm, hbm, hbm],
            out_specs=hbm,
            scratch_shapes=[
                pltpu.VMEM((T, D), bf16),
                pltpu.VMEM((Dl, FFl), bf16),
                pltpu.VMEM((FFl, Dl), bf16),
                pltpu.VMEM((Z, C * T, D), bf16),
                pltpu.VMEM((Y, D, B), bf16),
                pltpu.VMEM((F, Y * B, Dl), bf16),
                pltpu.VMEM((Z, C * T, Y * B), bf16),
                pltpu.VMEM((Z, F, C, T, Dl), bf16),
                pltpu.VMEM((Z, F, T, Dl), bf16),
                pltpu.VMEM((2, Z, F, T, Dl), bf16),
                pltpu.VMEM((Z, F, T, Dl), bf16),
                pltpu.VMEM((T, D), bf16),
                dma((5,)), dma((F,)),
                *[dma((2, Z)) for _ in range(6)],
                *[dma((2, Z, 2)) for _ in range(2)],
                dma((2, Z, 2)), dma((Z, 2)), dma((Z, 2)), dma((Z, 2)),
                dma((Z, F)), dma((Z, F)), dma((Z, F)), dma((2, Z, F)),
            ],
            compiler_params=pltpu.CompilerParams(
                collective_id=0, has_side_effects=True, vmem_limit_bytes=60 * 2**20),
        )(tokens, norm_gain.reshape(1, D), up_weight, down_weight)

    return jax.shard_map(
        on_device, mesh=mesh, in_specs=placed, out_specs=P(("fs", "tp"), None), check_vma=False)
```

```python
import functools
import math

import jax
import jax.numpy as jnp
from jax import lax
from jax.experimental import pallas as pl
from jax.experimental.pallas import tpu as pltpu
from jax.sharding import PartitionSpec as P

epsilon = 1e-06
MESH = pl.DeviceIdType.MESH
f32, bf16 = jnp.float32, jnp.bfloat16


def plain(tokens, norm_gain, up_weight, down_weight):
    values = tokens.astype(f32)
    mean_square = jnp.mean(values * values, axis=-1, keepdims=True)
    normed = (values * lax.rsqrt(mean_square + epsilon) * norm_gain).astype(bf16)
    up_whole = lax.all_gather(up_weight, "fs", axis=0, tiled=True)
    rows = lax.all_gather(normed, "tp", axis=0, tiled=True)
    preact = jnp.dot(rows, up_whole, preferred_element_type=f32)
    hidden = jnp.square(jnp.maximum(preact, 0.0)).astype(bf16)
    down_whole = lax.all_gather(down_weight, "fs", axis=1, tiled=True)
    partial_value = jnp.dot(hidden, down_whole, preferred_element_type=f32).astype(bf16)
    return lax.psum_scatter(partial_value, "tp", scatter_dimension=0, tiled=True)


PROGRAM = {
    0: [
        ("uown",), ("usend", 3), ("usend", 2), ("usend", 1), ("tsend",), ("dsend", 1),
        ("udiag", 0, 0), ("urel", 3, 0), ("udiag", 0, 1), ("urel", 3, 1), ("urel", 1, 0), ("udiag", 3, 0),
        ("urel", 1, 1), ("udiag", 3, 1), ("udiag", 1, 0), ("urel", 2, 0), ("udiag", 1, 1), ("urel", 2, 1),
        ("udiag", 2, 0), ("udiag", 2, 1),
        ("down_own",), ("drel", 1, 0), ("drel", 1, 1), ("trel", 1, 0), ("trel", 1, 1),
        ("uall", 0), ("uall", 1), ("uall", 3), ("uall", 2), ("hid", 0), ("hid", 1),
        ("dsend", 3), ("dsend", 2), ("ddiag", 0, 0), ("trel", 2, 0), ("ddiag", 0, 1),
        ("ddiag", 1, 0), ("dall", 0),
        ("proj", 0, (1, 0)), ("ddiag", 1, 1), ("sum", 1, 0), ("trel", 2, 1), ("drel", 3, 0), ("drel", 3, 1), ("hid", 2),
        ("proj", 0, (2,)), ("dall", 1), ("proj", 1, (2, 1, 0)), ("sum", 2, 0), ("sum", 2, 1), ("sum", 1, 1),
        ("trel", 3, 0), ("ddiag", 3, 0), ("ddiag", 3, 1), ("dall", 3),
        ("proj", 3, (2, 1, 0)), ("sum", 2, 3), ("sum", 1, 3),
        ("trel", 3, 1), ("drel", 2, 0), ("hid", 3), ("drel", 2, 1),
        ("proj", 0, (3,)), ("proj", 1, (3,)), ("sum", 3, 0), ("ddiag", 2, 0), ("proj", 3, (3,)), ("sum", 3, 1),
        ("sum", 3, 3), ("ddiag", 2, 1), ("dall", 2),
        ("proj", 2, (3,)), ("proj", 2, (2,)), ("sum", 3, 2), ("proj", 2, (1,)), ("sum", 2, 2),
        ("proj", 2, (0,)), ("sum", 1, 2),
        ("sum", 0, 3), ("sum", 0, 2), ("sum", 0, 0), ("sum", 0, 1),
    ],
    1: [
        ("uown",), ("usend", 2), ("usend", 3), ("usend", 0), ("tsend",), ("dsend", 0),
        ("udiag", 1, 0), ("udiag", 1, 1), ("urel", 3, 0), ("urel", 3, 1), ("udiag", 3, 0),
        ("urel", 0, 0), ("urel", 2, 0), ("udiag", 3, 1), ("urel", 0, 1), ("urel", 2, 1),
        ("udiag", 0, 0), ("udiag", 2, 0), ("trel", 0, 0), ("udiag", 0, 1), ("trel", 2, 0), ("trel", 0, 1),
        ("udiag", 2, 1), ("down_own",), ("trel", 2, 1), ("dsend", 2), ("dsend", 3), ("drel", 0, 0), ("drel", 0, 1),
        ("uall", 1), ("uall", 3), ("uall", 0), ("uall", 2),
        ("hid", 1), ("hid", 0), ("ddiag", 1, 0), ("trel", 3, 0), ("ddiag", 1, 1), ("hid", 2),
        ("ddiag", 0, 0), ("dall", 1), ("proj", 1, (2, 0, 1)), ("ddiag", 0, 1), ("drel", 3, 0), ("drel", 3, 1),
        ("trel", 3, 1), ("dall", 0), ("proj", 0, (2, 0, 1)), ("sum", 2, 0), ("drel", 2, 0), ("drel", 2, 1),
        ("hid", 3), ("ddiag", 3, 0), ("proj", 1, (3,)), ("proj", 0, (3,)), ("ddiag", 3, 1), ("sum", 2, 1),
        ("dall", 3), ("proj", 3, (2, 3, 0, 1)), ("sum", 2, 3), ("ddiag", 2, 0), ("ddiag", 2, 1),
        ("sum", 3, 0), ("sum", 3, 1), ("dall", 2), ("proj", 2, (0, 3, 2, 1)), ("sum", 0, 3), ("sum", 3, 3),
        ("sum", 0, 2), ("sum", 0, 0), ("sum", 3, 2), ("sum", 2, 2), ("sum", 0, 1),
        ("sum", 1, 0), ("sum", 1, 3), ("sum", 1, 1), ("sum", 1, 2),
    ],
}


def kernel(Z, X, Y, C, tok, gain, up, down, out,
           tokb, upb, downb, tokg, upg, downg, hid, part, cin, zin, zout, outb,
           in_s, out_s, wz_s, wz_r, wx_s, wx_r, wy_s, wy_r, wd_s, wd_r,
           t_s, t_r, tc_s, tc_r, rc_s, rc_r, rz_s, rz_r):
    T, D = tok.shape
    F = Z * X
    Dl = up.shape[0]
    B = upg.shape[2]
    fs, tp = lax.axis_index("fs"), lax.axis_index("tp")
    z, x = fs // X, fs % X
    y, c = tp // C, tp % C
    ox, oy, oc = X - 1 - x, Y - 1 - y, C - 1 - c
    low = z < Z // 2
    p = jnp.where(low, z, Z - 1 - z)
    side = jnp.where(low, 0, 1)

    def plane(q):
        return jnp.where(low, q, Z - 1 - q)

    def dev(zz=z, xx=x, yy=y, cc=c):
        return {"fs": zz * X + xx, "tp": yy * C + cc}

    def rcopy(src, dst, ss, rs, device):
        return pltpu.make_async_remote_copy(
            src_ref=src, dst_ref=dst, send_sem=ss, recv_sem=rs,
            device_id=device, device_id_type=MESH)

    def rows(start, size):
        return pl.ds(pl.multiple_of(start, size), size)

    barrier = pltpu.get_barrier_semaphore()
    peers = [dev(zz=(z + k) % Z) for k in range(1, Z)]
    peers += [dev(xx=ox), dev(yy=oy), dev(cc=oc)]
    for peer in peers:
        pl.semaphore_signal(barrier, inc=1, device_id=peer, device_id_type=MESH)

    loads = [
        pltpu.make_async_copy(tok, tokb, in_s.at[0]),
        pltpu.make_async_copy(up, upb, in_s.at[1]),
        pltpu.make_async_copy(down, downb, in_s.at[2]),
        pltpu.make_async_copy(up.at[:, rows(z * B, B)], upg.at[y, rows(fs * Dl, Dl)], in_s.at[3]),
        pltpu.make_async_copy(down.at[rows(z * B, B)], downg.at[fs, rows(y * B, B)], in_s.at[4]),
    ]
    for load in loads:
        load.start()
    loads[0].wait()
    RB = 32

    @pl.loop(0, T // RB)
    def _(i):
        v = tokb[rows(i * RB, RB), :].astype(f32)
        ms = jnp.mean(v * v, axis=-1, keepdims=True)
        tokg[z, rows(c * T + i * RB, RB), :] = (v * lax.rsqrt(ms + epsilon) * gain[...]).astype(bf16)

    for load in loads[1:]:
        load.wait()
    pl.semaphore_wait(barrier, len(peers))

    def piece(zz, xx, yy, k, half):
        f = zz * X + xx
        if k == 0:
            return upg.at[yy, rows(f * Dl + half * (Dl // 2), Dl // 2)]
        return downg.at[f, rows(yy * B + half * (B // 2), B // 2)]

    def own_piece(zz, k, half):
        if k == 0:
            return upb.at[rows(half * (Dl // 2), Dl // 2), rows(zz * B, B)]
        return downb.at[rows(zz * B + half * (B // 2), B // 2)]

    def wz(q, k, half):
        zz = plane(q)
        return rcopy(own_piece(zz, k, half), piece(z, x, y, k, half),
                     wz_s.at[k, zz, half], wz_r.at[k, z, half], dev(zz=zz))

    def wz_recv(q, k, half):
        zz = plane(q)
        ref = piece(zz, x, y, k, half)
        return rcopy(ref, ref, wz_s.at[k, zz, half], wz_r.at[k, zz, half], dev(zz=zz))

    def wx(q, k, half, xx=x):
        zz = plane(q)
        ref = piece(zz, xx, y, k, half)
        return rcopy(ref, ref, wx_s.at[k, zz, half], wx_r.at[k, zz, half], dev(xx=ox))

    def wy(q, k, half, yy=y):
        zz = plane(q)
        ref = piece(zz, x, yy, k, half)
        return rcopy(ref, ref, wy_s.at[k, zz, half], wy_r.at[k, zz, half], dev(yy=oy))

    def wd(q, k, half):
        zz = plane(q)
        ref = piece(zz, ox, y, k, 0) if half == 0 else piece(zz, x, oy, k, 1)
        to = dev(yy=oy) if half == 0 else dev(xx=ox)
        return rcopy(ref, ref, wd_s.at[k, zz, half], wd_r.at[k, zz, half], to)

    def wd_recv(q, k, half):
        zz = plane(q)
        ref = piece(zz, ox, oy, k, half)
        return rcopy(ref, ref, wd_s.at[k, zz, half], wd_r.at[k, zz, half], dev(yy=oy))

    TH = T // 2

    def tok_z(g, half, way):
        gg = plane(g)
        ref = tokg.at[gg, rows(c * T + half * TH, TH)]
        to = jnp.where(low, z + way, z - way)
        return rcopy(ref, ref, t_s.at[(way + 1) // 2, gg, half], t_r.at[gg, half], dev(zz=to))

    def tok_c(g, half, cc=c):
        gg = plane(g)
        ref = tokg.at[gg, rows(cc * T + half * TH, TH)]
        return rcopy(ref, ref, tc_s.at[gg, half], tc_r.at[gg, half], dev(cc=oc))

    NB = min(B, 256)

    def compute(g):
        gg = plane(g)
        for yy in range(Y):
            @pl.loop(0, B // NB)
            def _(j):
                h = jnp.dot(tokg[gg], upg[yy, :, rows(j * NB, NB)], preferred_element_type=f32)
                h = jnp.maximum(h, 0.0)
                hid[gg, :, rows(yy * B + j * NB, NB)] = (h * h).astype(bf16)

    def sum_c(gg, f):
        return rcopy(part.at[gg, f, oc], cin.at[gg, f], rc_s.at[gg, f], rc_r.at[gg, f], dev(cc=oc))

    def project(q, gs):
        for g in gs:
            gg = plane(g)

            @pl.loop(0, X)
            def _(xx):
                f = plane(q) * X + xx
                v = jnp.dot(hid[gg], downg[f], preferred_element_type=f32).astype(bf16)
                for cc in range(C):
                    part[gg, f, cc] = v[cc * T:(cc + 1) * T]
                sum_c(gg, f).start()

    def sum_z(gg, f, way):
        to = jnp.where(low, z + way, z - way)
        at = side if way > 0 else 1 - side
        return rcopy(zout.at[gg, f], zin.at[at, gg, f], rz_s.at[gg, f], rz_r.at[at, gg, f], dev(zz=to))

    def out_copy(f):
        cols = rows(f * Dl, Dl)
        return pltpu.make_async_copy(outb.at[:, cols], out.at[:, cols], out_s.at[f])

    def step(me, g, q):
        gg = plane(g)

        @pl.loop(0, X)
        def _(xx):
            f = plane(q) * X + xx
            sum_c(gg, f).wait_recv()
            acc = part[gg, f, c].astype(f32) + cin[gg, f].astype(f32)
            if me > 0 and g >= me:
                sum_z(gg, f, 1).wait_recv()
                acc = acc + zin[side, gg, f].astype(f32)
            if g <= me:
                sum_z(gg, f, -1).wait_recv()
                acc = acc + zin[1 - side, gg, f].astype(f32)
            if g == me:
                outb[:, rows(f * Dl, Dl)] = acc.astype(bf16)
                out_copy(f).start()
            else:
                zout[gg, f] = acc.astype(bf16)
                sum_z(gg, f, 1 if g > me else -1).start()

    def run(me, op, *args):
        k = 0 if op[0] == "u" else 1
        if op == "uown" or op == "down_own":
            for half in range(2):
                wx(me, k, half).start()
                wy(me, k, half).start()
        elif op == "usend" or op == "dsend":
            for half in range(2):
                wz(args[0], k, half).start()
        elif op == "urel" or op == "drel":
            q, half = args
            wz_recv(q, k, half).wait_recv()
            wx(q, k, half).start()
            wy(q, k, half).start()
        elif op == "udiag" or op == "ddiag":
            q, half = args
            if half == 0:
                wx(q, k, 0, ox).wait_recv()
            else:
                wy(q, k, 1, oy).wait_recv()
            wd(q, k, half).start()
        elif op == "uall" or op == "dall":
            q = args[0]
            wx(q, k, 1, ox).wait_recv()
            wy(q, k, 0, oy).wait_recv()
            for half in range(2):
                wd_recv(q, k, half).wait_recv()
        elif op == "tsend":
            for half in range(2):
                tok_z(me, half, 1).start()
                if me > 0:
                    tok_z(me, half, -1).start()
            for half in range(2):
                tok_c(me, half).start()
        elif op == "trel":
            g, half = args
            tok_z(g, half, 1 if g < me else -1).wait_recv()
            if me > 0:
                tok_z(g, half, 1 if g < me else -1).start()
            tok_c(g, half).start()
        elif op == "hid":
            for half in range(2):
                tok_c(args[0], half, oc).wait_recv()
            compute(args[0])
        elif op == "proj":
            project(*args)
        elif op == "sum":
            step(me, *args)

    def drain(me):
        for q in range(Z):
            for k in range(2):
                for half in range(2):
                    if q != me:
                        wz(q, k, half).wait_send()
                    wx(q, k, half).wait_send()
                    wy(q, k, half).wait_send()
                    wd(q, k, half).wait_send()
            for half in range(2):
                tok_c(q, half).wait_send()
                if q == me or me > 0:
                    if q <= me:
                        tok_z(q, half, 1).wait_send()
                    if q >= me and me > 0:
                        tok_z(q, half, -1).wait_send()

    for me in range(Z // 2):
        @pl.when(p == me)
        def _(me=me):
            for item in PROGRAM[me]:
                run(me, *item)
            drain(me)

    @pl.loop(0, F)
    def _(f):
        @pl.loop(0, Z)
        def _(gg):
            sum_c(gg, f).wait_send()

            @pl.when(gg != z)
            def _():
                sum_z(gg, f, 1).wait_send()
        out_copy(f).wait()


def solution(mesh):
    n_fs, n_tp = mesh.shape["fs"], mesh.shape["tp"]
    X = 2 ** (int(math.log2(n_fs)) // 2)
    Z = n_fs // X
    C = 2
    Y = n_tp // C
    placed = (P(("fs", "tp"), None), P(), P("fs", "tp"), P("tp", "fs"))

    def on_device(tokens, norm_gain, up_weight, down_weight):
        T, D = tokens.shape
        Dl, FFl = up_weight.shape
        B = FFl // Z
        if X != 2 or Y != 2 or Z != 4 or Z * X != n_fs or Dl % 256 or B % 256 or T % 32:
            return plain(tokens, norm_gain, up_weight, down_weight)
        F = Z * X
        dma = pltpu.SemaphoreType.DMA
        vm = pl.BlockSpec(memory_space=pltpu.VMEM)
        hbm = pl.BlockSpec(memory_space=pl.ANY)
        return pl.pallas_call(
            functools.partial(kernel, Z, X, Y, C),
            out_shape=jax.ShapeDtypeStruct((T, D), bf16),
            in_specs=[hbm, vm, hbm, hbm],
            out_specs=hbm,
            scratch_shapes=[
                pltpu.VMEM((T, D), bf16),
                pltpu.VMEM((Dl, FFl), bf16),
                pltpu.VMEM((FFl, Dl), bf16),
                pltpu.VMEM((Z, C * T, D), bf16),
                pltpu.VMEM((Y, D, B), bf16),
                pltpu.VMEM((F, Y * B, Dl), bf16),
                pltpu.VMEM((Z, C * T, Y * B), bf16),
                pltpu.VMEM((Z, F, C, T, Dl), bf16),
                pltpu.VMEM((Z, F, T, Dl), bf16),
                pltpu.VMEM((2, Z, F, T, Dl), bf16),
                pltpu.VMEM((Z, F, T, Dl), bf16),
                pltpu.VMEM((T, D), bf16),
                dma((5,)), dma((F,)),
                *[dma((2, Z, 2)) for _ in range(8)],
                dma((2, Z, 2)), dma((Z, 2)), dma((Z, 2)), dma((Z, 2)),
                dma((Z, F)), dma((Z, F)), dma((Z, F)), dma((2, Z, F)),
            ],
            compiler_params=pltpu.CompilerParams(
                collective_id=0, has_side_effects=True, vmem_limit_bytes=60 * 2**20),
        )(tokens, norm_gain.reshape(1, D), up_weight, down_weight)

    return jax.shard_map(
        on_device, mesh=mesh, in_specs=placed, out_specs=P(("fs", "tp"), None), check_vma=False)
```

```python
import functools
import math

import jax
import jax.numpy as jnp
from jax import lax
from jax.experimental import pallas as pl
from jax.experimental.pallas import tpu as pltpu
from jax.sharding import PartitionSpec as P

epsilon = 1e-06
MESH = pl.DeviceIdType.MESH
CUTS = 4
f32, bf16 = jnp.float32, jnp.bfloat16


def plain(tokens, norm_gain, up_weight, down_weight):
    values = tokens.astype(f32)
    mean_square = jnp.mean(values * values, axis=-1, keepdims=True)
    normed = (values * lax.rsqrt(mean_square + epsilon) * norm_gain).astype(bf16)
    up_whole = lax.all_gather(up_weight, "fs", axis=0, tiled=True)
    rows = lax.all_gather(normed, "tp", axis=0, tiled=True)
    preact = jnp.dot(rows, up_whole, preferred_element_type=f32)
    hidden = jnp.square(jnp.maximum(preact, 0.0)).astype(bf16)
    down_whole = lax.all_gather(down_weight, "fs", axis=1, tiled=True)
    partial_value = jnp.dot(hidden, down_whole, preferred_element_type=f32).astype(bf16)
    return lax.psum_scatter(partial_value, "tp", scatter_dimension=0, tiled=True)


PROGRAM = {
    0: [
        ("uown",), ("usend", 3, 1), ("usend", 1, 1), ("norm",), ("down_own",), ("tsend", 0, 1), ("tsend", 2, 1),
        ("urel", 3, 1), ("dsend", 3, 1), ("urel", 2, 1), ("usend", 1, 0), ("ddiag", 0, 1), ("ddiag", 0, 0),
        ("dsend", 1, 0), ("dsend", 3, 0), ("usend", 2, 0), ("dsend", 2, 1), ("udiag", 0, 0), ("tsend", 1, 0),
        ("urel", 2, 0), ("drel", 3, 1), ("usend", 3, 0), ("urel", 1, 0), ("udiag", 3, 1), ("drel", 3, 0),
        ("urel", 1, 1), ("usend", 2, 1), ("udiag", 2, 0), ("tsend", 3, 1), ("urel", 3, 0), ("trel", 1, 1),
        ("tsend", 1, 1), ("udiag", 0, 1), ("ddiag", 3, 0), ("udiag", 2, 1), ("tsend", 3, 0), ("udiag", 1, 0),
        ("dall", 0), ("udiag", 3, 0), ("ddiag", 3, 1), ("udiag", 1, 1), ("trel", 1, 2), ("trel", 2, 0),
        ("dsend", 1, 1), ("tsend", 0, 0), ("trel", 1, 3), ("trel", 2, 3), ("dall", 3), ("drel", 1, 0),
        ("dsend", 2, 0), ("drel", 1, 1), ("trel", 2, 2), ("uall", 1), ("uall", 2), ("trel", 1, 0), ("uall", 3),
        ("uall", 0), ("trel", 2, 1), ("hid", 2), ("proj", 3, 2), ("ddiag", 1, 0), ("proj", 0, 2), ("hid", 1),
        ("ddiag", 1, 1), ("tsend", 2, 0), ("sum", 2, 3), ("proj", 3, 1), ("sum", 1, 3), ("sum", 2, 0), ("trel", 3, 1),
        ("trel", 3, 3), ("trel", 3, 2), ("hid", 0), ("drel", 2, 0), ("dall", 1), ("proj", 1, 2), ("trel", 3, 0),
        ("sum", 2, 1), ("hid", 3), ("drel", 2, 1), ("proj", 3, 3), ("sum", 3, 3), ("ddiag", 2, 0), ("proj", 1, 3),
        ("ddiag", 2, 1), ("sum", 3, 1), ("proj", 0, 3), ("proj", 0, 1), ("sum", 3, 0), ("dall", 2), ("proj", 2, 3),
        ("sum", 3, 2), ("sum", 1, 0), ("proj", 3, 0), ("proj", 1, 1), ("proj", 2, 2), ("proj", 2, 1), ("sum", 2, 2),
        ("sum", 1, 1), ("proj", 2, 0), ("sum", 1, 2), ("proj", 1, 0), ("proj", 0, 0), ("sum", 0, 0), ("sum", 0, 2),
        ("sum", 0, 3), ("sum", 0, 1),
    ],
    1: [
        ("uown",), ("usend", 3, 1), ("usend", 2, 1), ("usend", 3, 0), ("usend", 2, 0), ("usend", 0, 1),
        ("usend", 0, 0), ("norm",), ("tsend", 0, 0), ("down_own",), ("urel", 2, 1), ("tsend", 1, 1), ("dsend", 0, 1),
        ("tsend", 3, 1), ("tsend", 0, 1), ("urel", 0, 1), ("tsend", 2, -1), ("urel", 2, 0), ("tsend", 2, 0),
        ("tsend", 2, 1), ("tsend", 1, -1), ("urel", 0, 0), ("udiag", 2, 1), ("udiag", 0, 1), ("drel", 0, 0),
        ("trel", 2, 1), ("tsend", 3, -1), ("dsend", 0, 0), ("urel", 3, 0), ("ddiag", 1, 0), ("tsend", 3, 0),
        ("udiag", 1, 0), ("urel", 3, 1), ("udiag", 1, 1), ("trel", 2, 3), ("tsend", 1, 0), ("drel", 3, 1),
        ("udiag", 0, 0), ("trel", 2, 0), ("trel", 0, 3), ("trel", 0, 2), ("tsend", 0, -1), ("trel", 0, 1),
        ("uall", 1), ("udiag", 2, 0), ("trel", 2, 2), ("ddiag", 1, 1), ("dsend", 2, 0), ("uall", 2), ("trel", 0, 0),
        ("dall", 1), ("ddiag", 0, 0), ("dsend", 3, 0), ("udiag", 3, 0), ("trel", 3, 2), ("ddiag", 3, 1),
        ("udiag", 3, 1), ("trel", 3, 3), ("drel", 3, 0), ("drel", 0, 1), ("trel", 3, 1), ("uall", 0), ("dsend", 2, 1),
        ("uall", 3), ("hid", 1), ("hid", 2), ("trel", 3, 0), ("ddiag", 3, 0), ("hid", 3), ("dsend", 3, 1),
        ("ddiag", 0, 1), ("drel", 2, 0), ("drel", 2, 1), ("dall", 3), ("proj", 3, 2), ("proj", 1, 3), ("proj", 1, 2),
        ("hid", 0), ("proj", 3, 3), ("sum", 2, 3), ("proj", 1, 1), ("proj", 3, 0), ("ddiag", 2, 1), ("sum", 2, 1),
        ("dall", 0), ("proj", 0, 0), ("ddiag", 2, 0), ("proj", 3, 1), ("proj", 0, 2), ("proj", 0, 1), ("sum", 3, 3),
        ("sum", 3, 1), ("proj", 0, 3), ("dall", 2), ("proj", 2, 3), ("proj", 2, 2), ("sum", 0, 0), ("sum", 3, 0),
        ("proj", 1, 0), ("proj", 2, 0), ("sum", 0, 2), ("sum", 3, 2), ("sum", 2, 0), ("sum", 0, 3), ("proj", 2, 1),
        ("sum", 0, 1), ("sum", 2, 2), ("sum", 1, 3), ("sum", 1, 0), ("sum", 1, 1), ("sum", 1, 2),
    ],
}


def kernel(Z, X, Y, C, tok, gain, up, down, out,
           tokb, upb, downb, tokg, upg, downg, hid, part, cin, zin, zout,
           in_s, wz_s, wz_r, wx_s, wx_r, wy_s, wy_r, wd_s, wd_r,
           t_s, t_r, tc_s, tc_r, rc_s, rc_r, rz_s, rz_r):
    T, D = tok.shape
    F = Z * X
    Dl = up.shape[0]
    B = upg.shape[2]
    fs, tp = lax.axis_index("fs"), lax.axis_index("tp")
    z, x = fs // X, fs % X
    y, c = tp // C, tp % C
    ox, oy, oc = X - 1 - x, Y - 1 - y, C - 1 - c
    low = z < Z // 2
    p = jnp.where(low, z, Z - 1 - z)
    side = jnp.where(low, 0, 1)

    def plane(q):
        return jnp.where(low, q, Z - 1 - q)

    def dev(zz=z, xx=x, yy=y, cc=c):
        return {"fs": zz * X + xx, "tp": yy * C + cc}

    def rcopy(src, dst, ss, rs, device):
        return pltpu.make_async_remote_copy(
            src_ref=src, dst_ref=dst, send_sem=ss, recv_sem=rs,
            device_id=device, device_id_type=MESH)

    def rows(start, size):
        return pl.ds(pl.multiple_of(start, size), size)

    barrier = pltpu.get_barrier_semaphore()
    peers = [dev(zz=(z + k) % Z) for k in range(1, Z)]
    peers += [dev(xx=ox), dev(yy=oy), dev(cc=oc)]
    for peer in peers:
        pl.semaphore_signal(barrier, inc=1, device_id=peer, device_id_type=MESH)

    loads = [
        pltpu.make_async_copy(up, upb, in_s.at[0]),
        pltpu.make_async_copy(tok, tokb, in_s.at[1]),
        pltpu.make_async_copy(down, downb, in_s.at[2]),
        pltpu.make_async_copy(up.at[:, rows(z * B, B)], upg.at[y, rows(fs * Dl, Dl)], in_s.at[3]),
        pltpu.make_async_copy(down.at[rows(z * B, B)], downg.at[fs, rows(y * B, B)], in_s.at[4]),
    ]
    for load in loads:
        load.start()
    loads[0].wait()
    loads[3].wait()
    pl.semaphore_wait(barrier, len(peers))

    def normalize():
        loads[1].wait()
        RB = 32

        @pl.loop(0, T // RB)
        def _(i):
            v = tokb[rows(i * RB, RB), :].astype(f32)
            ms = jnp.mean(v * v, axis=-1, keepdims=True)
            tokg[z, rows(c * T + i * RB, RB), :] = (v * lax.rsqrt(ms + epsilon) * gain[...]).astype(bf16)

        loads[2].wait()
        loads[4].wait()

    def piece(zz, xx, yy, k, half):
        f = zz * X + xx
        if k == 0:
            return upg.at[yy, rows(f * Dl + half * (Dl // 2), Dl // 2)]
        return downg.at[f, rows(yy * B + half * (B // 2), B // 2)]

    def own_piece(zz, k, half):
        if k == 0:
            return upb.at[rows(half * (Dl // 2), Dl // 2), rows(zz * B, B)]
        return downb.at[rows(zz * B + half * (B // 2), B // 2)]

    def wz(q, k, half):
        zz = plane(q)
        return rcopy(own_piece(zz, k, half), piece(z, x, y, k, half),
                     wz_s.at[k, zz, half], wz_r.at[k, z, half], dev(zz=zz))

    def wz_recv(q, k, half):
        zz = plane(q)
        ref = piece(zz, x, y, k, half)
        return rcopy(ref, ref, wz_s.at[k, zz, half], wz_r.at[k, zz, half], dev(zz=zz))

    def wx(q, k, half, xx=x):
        zz = plane(q)
        ref = piece(zz, xx, y, k, half)
        return rcopy(ref, ref, wx_s.at[k, zz, half], wx_r.at[k, zz, half], dev(xx=ox))

    def wy(q, k, half, yy=y):
        zz = plane(q)
        ref = piece(zz, x, yy, k, half)
        return rcopy(ref, ref, wy_s.at[k, zz, half], wy_r.at[k, zz, half], dev(yy=oy))

    def wd(q, k, half):
        zz = plane(q)
        ref = piece(zz, ox, y, k, 0) if half == 0 else piece(zz, x, oy, k, 1)
        to = dev(yy=oy) if half == 0 else dev(xx=ox)
        return rcopy(ref, ref, wd_s.at[k, zz, half], wd_r.at[k, zz, half], to)

    def wd_recv(q, k, half):
        zz = plane(q)
        ref = piece(zz, ox, oy, k, half)
        return rcopy(ref, ref, wd_s.at[k, zz, half], wd_r.at[k, zz, half], dev(yy=oy))

    TC = T // CUTS

    def tok_z(g, cut, way):
        gg = plane(g)
        ref = tokg.at[gg, rows(c * T + cut * TC, TC)]
        to = jnp.where(low, z + way, z - way)
        return rcopy(ref, ref, t_s.at[(way + 1) // 2, gg, cut], t_r.at[gg, cut], dev(zz=to))

    def tok_c(g, cut, cc=c):
        gg = plane(g)
        ref = tokg.at[gg, rows(cc * T + cut * TC, TC)]
        return rcopy(ref, ref, tc_s.at[gg, cut], tc_r.at[gg, cut], dev(cc=oc))

    NB = min(B, 512)

    def compute(g):
        gg = plane(g)
        for yy in range(Y):
            for j in range(B // NB):
                h = jnp.dot(tokg[gg], upg[yy, :, rows(j * NB, NB)], preferred_element_type=f32)
                h = jnp.maximum(h, 0.0)
                hid[gg, :, rows(yy * B + j * NB, NB)] = (h * h).astype(bf16)

    def sum_c(gg, f):
        return rcopy(part.at[gg, f, oc], cin.at[gg, f], rc_s.at[gg, f], rc_r.at[gg, f], dev(cc=oc))

    def project(q, g):
        gg = plane(g)

        @pl.loop(0, X)
        def _(xx):
            f = plane(q) * X + xx
            v = jnp.dot(hid[gg], downg[f], preferred_element_type=f32).astype(bf16)
            for cc in range(C):
                part[gg, f, cc] = v[cc * T:(cc + 1) * T]
            sum_c(gg, f).start()

    def sum_z(gg, f, way):
        to = jnp.where(low, z + way, z - way)
        at = side if way > 0 else 1 - side
        return rcopy(zout.at[gg, f], zin.at[at, gg, f], rz_s.at[gg, f], rz_r.at[at, gg, f], dev(zz=to))

    def step(me, g, q):
        gg = plane(g)

        @pl.loop(0, X)
        def _(xx):
            f = plane(q) * X + xx
            sum_c(gg, f).wait_recv()
            acc = part[gg, f, c].astype(f32) + cin[gg, f].astype(f32)
            if me > 0 and g >= me:
                sum_z(gg, f, 1).wait_recv()
                acc = acc + zin[side, gg, f].astype(f32)
            if g <= me:
                sum_z(gg, f, -1).wait_recv()
                acc = acc + zin[1 - side, gg, f].astype(f32)
            if g == me:
                out[:, rows(f * Dl, Dl)] = acc.astype(bf16)
            else:
                zout[gg, f] = acc.astype(bf16)
                sum_z(gg, f, 1 if g > me else -1).start()

    def run(me, op, *args):
        k = 0 if op[0] == "u" else 1
        if op == "norm":
            normalize()
        elif op == "uown" or op == "down_own":
            for half in range(2):
                wx(me, k, half).start()
                wy(me, k, half).start()
        elif op == "usend" or op == "dsend":
            wz(args[0], k, args[1]).start()
        elif op == "urel" or op == "drel":
            q, half = args
            wz_recv(q, k, half).wait_recv()
            wx(q, k, half).start()
            wy(q, k, half).start()
        elif op == "udiag" or op == "ddiag":
            q, half = args
            if half == 0:
                wx(q, k, 0, ox).wait_recv()
            else:
                wy(q, k, 1, oy).wait_recv()
            wd(q, k, half).start()
        elif op == "uall" or op == "dall":
            q = args[0]
            wx(q, k, 1, ox).wait_recv()
            wy(q, k, 0, oy).wait_recv()
            for half in range(2):
                wd_recv(q, k, half).wait_recv()
        elif op == "tsend":
            cut, way = args
            if way == 0:
                tok_c(me, cut).start()
            else:
                tok_z(me, cut, way).start()
        elif op == "trel":
            g, cut = args
            tok_z(g, cut, 1 if g < me else -1).wait_recv()
            if me > 0:
                tok_z(g, cut, 1 if g < me else -1).start()
            tok_c(g, cut).start()
        elif op == "hid":
            for cut in range(CUTS):
                tok_c(args[0], cut, oc).wait_recv()
            compute(args[0])
        elif op == "proj":
            project(*args)
        elif op == "sum":
            step(me, *args)

    def drain(me):
        for q in range(Z):
            for k in range(2):
                for half in range(2):
                    if q != me:
                        wz(q, k, half).wait_send()
                    wx(q, k, half).wait_send()
                    wy(q, k, half).wait_send()
                    wd(q, k, half).wait_send()
            for cut in range(CUTS):
                tok_c(q, cut).wait_send()
                if q <= me:
                    tok_z(q, cut, 1).wait_send()
                if q >= me and me > 0:
                    tok_z(q, cut, -1).wait_send()

    for me in range(Z // 2):
        @pl.when(p == me)
        def _(me=me):
            for item in PROGRAM[me]:
                run(me, *item)
            drain(me)

    @pl.loop(0, F)
    def _(f):
        @pl.loop(0, Z)
        def _(gg):
            sum_c(gg, f).wait_send()

            @pl.when(gg != z)
            def _():
                sum_z(gg, f, 1).wait_send()


def solution(mesh):
    n_fs, n_tp = mesh.shape["fs"], mesh.shape["tp"]
    X = 2 ** (int(math.log2(n_fs)) // 2)
    Z = n_fs // X
    C = 2
    Y = n_tp // C
    placed = (P(("fs", "tp"), None), P(), P("fs", "tp"), P("tp", "fs"))

    def on_device(tokens, norm_gain, up_weight, down_weight):
        T, D = tokens.shape
        Dl, FFl = up_weight.shape
        B = FFl // Z
        if X != 2 or Y != 2 or Z != 4 or Z * X != n_fs or Dl % 256 or B % 256 or T % (16 * CUTS):
            return plain(tokens, norm_gain, up_weight, down_weight)
        F = Z * X
        dma = pltpu.SemaphoreType.DMA
        vm = pl.BlockSpec(memory_space=pltpu.VMEM)
        hbm = pl.BlockSpec(memory_space=pltpu.HBM)
        return pl.pallas_call(
            functools.partial(kernel, Z, X, Y, C),
            out_shape=jax.ShapeDtypeStruct((T, D), bf16),
            in_specs=[hbm, vm, hbm, hbm],
            out_specs=vm,
            scratch_shapes=[
                pltpu.VMEM((T, D), bf16),
                pltpu.VMEM((Dl, FFl), bf16),
                pltpu.VMEM((FFl, Dl), bf16),
                pltpu.VMEM((Z, C * T, D), bf16),
                pltpu.VMEM((Y, D, B), bf16),
                pltpu.VMEM((F, Y * B, Dl), bf16),
                pltpu.VMEM((Z, C * T, Y * B), bf16),
                pltpu.VMEM((Z, F, C, T, Dl), bf16),
                pltpu.VMEM((Z, F, T, Dl), bf16),
                pltpu.VMEM((2, Z, F, T, Dl), bf16),
                pltpu.VMEM((Z, F, T, Dl), bf16),
                dma((5,)),
                *[dma((2, Z, 2)) for _ in range(8)],
                dma((2, Z, CUTS)), *[dma((Z, CUTS)) for _ in range(3)],
                dma((Z, F)), dma((Z, F)), dma((Z, F)), dma((2, Z, F)),
            ],
            compiler_params=pltpu.CompilerParams(
                collective_id=0, has_side_effects=True, vmem_limit_bytes=53 * 2**20),
        )(tokens, norm_gain.reshape(1, D), up_weight, down_weight)

    return jax.shard_map(
        on_device, mesh=mesh, in_specs=placed, out_specs=P(("fs", "tp"), None), check_vma=False)
```

```python
import functools
import math

import jax
import jax.numpy as jnp
from jax import lax
from jax.experimental import pallas as pl
from jax.experimental.pallas import tpu as pltpu
from jax.sharding import PartitionSpec as P

epsilon = 1e-06
MESH = pl.DeviceIdType.MESH
CUTS = 4
f32, bf16 = jnp.float32, jnp.bfloat16


def plain(tokens, norm_gain, up_weight, down_weight):
    values = tokens.astype(f32)
    mean_square = jnp.mean(values * values, axis=-1, keepdims=True)
    normed = (values * lax.rsqrt(mean_square + epsilon) * norm_gain).astype(bf16)
    up_whole = lax.all_gather(up_weight, "fs", axis=0, tiled=True)
    rows = lax.all_gather(normed, "tp", axis=0, tiled=True)
    preact = jnp.dot(rows, up_whole, preferred_element_type=f32)
    hidden = jnp.square(jnp.maximum(preact, 0.0)).astype(bf16)
    down_whole = lax.all_gather(down_weight, "fs", axis=1, tiled=True)
    partial_value = jnp.dot(hidden, down_whole, preferred_element_type=f32).astype(bf16)
    return lax.psum_scatter(partial_value, "tp", scatter_dimension=0, tiled=True)


PROGRAM = {
    0: [
        ("usend", 1, 0), ("usend", 3, 1), ("uown",), ("norm",), ("usend", 2, 1), ("down_own",), ("usend", 3, 0),
        ("urel", 3, 1), ("tsend", 0, 1), ("tsend", 3, 1), ("usend", 1, 1), ("urel", 2, 1), ("tsend", 0, 0),
        ("dsend", 1, 0), ("usend", 2, 0), ("dsend", 1, 1), ("dsend", 2, 1), ("tsend", 1, 1), ("urel", 3, 0),
        ("urel", 1, 0), ("urel", 1, 1), ("trel", 1, 1), ("drel", 1, 1), ("ddiag", 0, 0), ("urel", 2, 0),
        ("udiag", 1, 1), ("udiag", 0, 0), ("drel", 1, 0), ("dsend", 2, 0), ("tsend", 2, 1), ("udiag", 2, 1),
        ("udiag", 3, 1), ("udiag", 3, 0), ("dsend", 3, 0), ("udiag", 1, 0), ("udiag", 0, 1), ("ddiag", 1, 1),
        ("ddiag", 1, 0), ("ddiag", 0, 1), ("udiag", 2, 0), ("dsend", 3, 1), ("uall", 1), ("uall", 3), ("trel", 1, 3),
        ("trel", 1, 0), ("trel", 1, 2), ("trel", 3, 3), ("drel", 3, 1), ("uall", 2), ("dall", 0), ("uall", 0),
        ("drel", 3, 0), ("hid", 1), ("trel", 3, 0), ("dall", 1), ("proj", 1, 1), ("trel", 3, 2), ("proj", 0, 1),
        ("trel", 3, 1), ("ddiag", 3, 1), ("sum", 1, 0), ("hid", 3), ("ddiag", 3, 0), ("sum", 1, 1), ("proj", 1, 3),
        ("drel", 2, 1), ("proj", 0, 3), ("sum", 3, 0), ("drel", 2, 0), ("sum", 3, 1), ("dall", 3), ("proj", 3, 1),
        ("tsend", 2, 0), ("trel", 2, 3), ("proj", 3, 3), ("sum", 3, 3), ("trel", 2, 1), ("tsend", 1, 0),
        ("ddiag", 2, 1), ("trel", 2, 2), ("trel", 2, 0), ("ddiag", 2, 0), ("sum", 1, 3), ("hid", 2), ("proj", 3, 2),
        ("sum", 2, 3), ("tsend", 3, 0), ("dall", 2), ("proj", 0, 2), ("sum", 2, 0), ("proj", 2, 2), ("proj", 2, 3),
        ("hid", 0), ("proj", 3, 0), ("sum", 3, 2), ("sum", 2, 2), ("proj", 1, 2), ("sum", 2, 1), ("proj", 2, 1),
        ("proj", 0, 0), ("sum", 0, 0), ("sum", 0, 3), ("proj", 1, 0), ("proj", 2, 0), ("sum", 1, 2), ("sum", 0, 2),
        ("sum", 0, 1),
    ],
    1: [
        ("uown",), ("usend", 3, 1), ("usend", 0, 0), ("usend", 3, 0), ("usend", 2, 1), ("norm",), ("tsend", 1, -1),
        ("down_own",), ("urel", 3, 1), ("trel", 0, 0), ("usend", 0, 1), ("urel", 0, 0), ("udiag", 1, 1),
        ("urel", 2, 1), ("dsend", 0, 1), ("dsend", 0, 0), ("udiag", 3, 1), ("udiag", 1, 0), ("tsend", 0, -1),
        ("ddiag", 1, 1), ("trel", 0, 3), ("tsend", 3, 1), ("trel", 3, 0), ("urel", 0, 1), ("usend", 2, 0),
        ("ddiag", 1, 0), ("trel", 2, 3), ("tsend", 3, 0), ("drel", 0, 1), ("tsend", 3, -1), ("drel", 0, 0),
        ("udiag", 0, 0), ("trel", 3, 3), ("trel", 0, 1), ("urel", 3, 0), ("trel", 0, 2), ("udiag", 0, 1),
        ("urel", 2, 0), ("tsend", 2, -1), ("tsend", 1, 1), ("trel", 3, 1), ("tsend", 0, 1), ("dsend", 3, 1),
        ("udiag", 3, 0), ("drel", 3, 1), ("udiag", 2, 0), ("udiag", 2, 1), ("ddiag", 0, 0), ("trel", 3, 2),
        ("dsend", 3, 0), ("tsend", 1, 0), ("uall", 1), ("ddiag", 0, 1), ("tsend", 2, 1), ("trel", 2, 0),
        ("tsend", 0, 0), ("uall", 2), ("uall", 3), ("dall", 1), ("drel", 3, 0), ("trel", 2, 1), ("uall", 0),
        ("dsend", 2, 1), ("tsend", 2, 0), ("hid", 3), ("hid", 0), ("dall", 0), ("ddiag", 3, 0), ("proj", 0, 0),
        ("ddiag", 3, 1), ("dsend", 2, 0), ("proj", 0, 3), ("proj", 1, 3), ("trel", 2, 2), ("hid", 1), ("dall", 3),
        ("drel", 2, 1), ("proj", 0, 1), ("sum", 3, 0), ("proj", 3, 3), ("drel", 2, 0), ("sum", 3, 1), ("hid", 2),
        ("proj", 3, 0), ("sum", 3, 3), ("ddiag", 2, 0), ("ddiag", 2, 1), ("sum", 0, 3), ("proj", 3, 2),
        ("proj", 1, 2), ("proj", 0, 2), ("sum", 0, 0), ("sum", 2, 3), ("dall", 2), ("proj", 2, 0), ("proj", 1, 0),
        ("proj", 2, 3), ("sum", 2, 0), ("sum", 0, 2), ("proj", 2, 2), ("sum", 3, 2), ("sum", 2, 2), ("proj", 1, 1),
        ("proj", 2, 1), ("proj", 3, 1), ("sum", 0, 1), ("sum", 2, 1), ("sum", 1, 0), ("sum", 1, 3), ("sum", 1, 1),
        ("sum", 1, 2),
    ],
}


def kernel(Z, X, Y, C, tok, gain, up, down, out,
           tokb, upb, downb, tokg, upg, downg, hid, part, cin, zin, zout,
           in_s, wz_s, wx_s, wy_s, wd_s, t_s, tc_s, rc_s, rz_s,
           wz_r, wx_r, wy_r, all_r, t_r, tc_r, rc_r, rz_r):
    T, D = tok.shape
    F = Z * X
    Dl = up.shape[0]
    B = upg.shape[2]
    fs, tp = lax.axis_index("fs"), lax.axis_index("tp")
    z, x = fs // X, fs % X
    y, c = tp // C, tp % C
    ox, oy, oc = X - 1 - x, Y - 1 - y, C - 1 - c
    low = z < Z // 2
    p = jnp.where(low, z, Z - 1 - z)

    def plane(q):
        return jnp.where(low, q, Z - 1 - q)

    def dev(zz=z, xx=x, yy=y, cc=c):
        return {"fs": zz * X + xx, "tp": yy * C + cc}

    def rcopy(src, dst, ss, rs, device):
        return pltpu.make_async_remote_copy(
            src_ref=src, dst_ref=dst, send_sem=ss, recv_sem=rs,
            device_id=device, device_id_type=MESH)

    def rows(start, size):
        return pl.ds(pl.multiple_of(start, size), size)

    barrier = pltpu.get_barrier_semaphore()
    peers = [dev(zz=(z + k) % Z) for k in range(1, Z)]
    peers += [dev(xx=ox), dev(yy=oy), dev(cc=oc)]
    for peer in peers:
        pl.semaphore_signal(barrier, inc=1, device_id=peer, device_id_type=MESH)

    loads = [
        pltpu.make_async_copy(up, upb, in_s.at[0]),
        pltpu.make_async_copy(up.at[:, rows(z * B, B)], upg.at[y, rows(fs * Dl, Dl)], in_s.at[1]),
        pltpu.make_async_copy(tok, tokb, in_s.at[2]),
        pltpu.make_async_copy(down, downb, in_s.at[3]),
        pltpu.make_async_copy(down.at[rows(z * B, B)], downg.at[fs, rows(y * B, B)], in_s.at[4]),
    ]
    for load in loads[:3]:
        load.start()
    loads[0].wait()
    for load in loads[3:]:
        load.start()
    loads[1].wait()
    pl.semaphore_wait(barrier, len(peers))

    def normalize():
        loads[2].wait()
        RB = 32

        @pl.loop(0, T // RB)
        def _(i):
            v = tokb[rows(i * RB, RB), :].astype(f32)
            ms = jnp.mean(v * v, axis=-1, keepdims=True)
            tokg[z, rows(c * T + i * RB, RB), :] = (v * lax.rsqrt(ms + epsilon) * gain[...]).astype(bf16)

        loads[3].wait()
        loads[4].wait()

    def piece(zz, xx, yy, k, half):
        f = zz * X + xx
        if k == 0:
            return upg.at[yy, rows(f * Dl + half * (Dl // 2), Dl // 2)]
        return downg.at[f, rows(yy * B + half * (B // 2), B // 2)]

    def own_piece(zz, k, half):
        if k == 0:
            return upb.at[rows(half * (Dl // 2), Dl // 2), rows(zz * B, B)]
        return downb.at[rows(zz * B + half * (B // 2), B // 2)]

    def wz(q, k, half):
        zz = plane(q)
        return rcopy(own_piece(zz, k, half), piece(z, x, y, k, half),
                     wz_s.at[0], wz_r.at[k, z, half], dev(zz=zz))

    def wz_recv(q, k, half):
        zz = plane(q)
        ref = piece(zz, x, y, k, half)
        return rcopy(ref, ref, wz_s.at[0], wz_r.at[k, zz, half], dev(zz=zz))

    def wx(q, k, half, xx=x):
        zz = plane(q)
        ref = piece(zz, xx, y, k, half)
        rs = wx_r.at[k, zz] if half == 0 else all_r.at[k, zz]
        return rcopy(ref, ref, wx_s.at[0], rs, dev(xx=ox))

    def wy(q, k, half, yy=y):
        zz = plane(q)
        ref = piece(zz, x, yy, k, half)
        rs = wy_r.at[k, zz] if half == 1 else all_r.at[k, zz]
        return rcopy(ref, ref, wy_s.at[0], rs, dev(yy=oy))

    def wd(q, k, half):
        zz = plane(q)
        ref = piece(zz, ox, y, k, 0) if half == 0 else piece(zz, x, oy, k, 1)
        to = dev(yy=oy) if half == 0 else dev(xx=ox)
        return rcopy(ref, ref, wd_s.at[0], all_r.at[k, zz], to)

    def rest_recv(q, k):
        zz = plane(q)
        ref = upg.at[y, pl.ds(0, 2 * Dl)] if k == 0 else downg.at[zz * X]
        return rcopy(ref, ref, wd_s.at[0], all_r.at[k, zz], dev(yy=oy))

    TC = T // CUTS

    def tok_z(g, cut, way):
        gg = plane(g)
        ref = tokg.at[gg, rows(c * T + cut * TC, TC)]
        to = jnp.where(low, z + way, z - way)
        return rcopy(ref, ref, t_s.at[0], t_r.at[gg, cut], dev(zz=to))

    def tok_c(g, cut, cc=c):
        gg = plane(g)
        ref = tokg.at[gg, rows(cc * T + cut * TC, TC)]
        return rcopy(ref, ref, tc_s.at[0], tc_r.at[gg], dev(cc=oc))

    NB = min(B, 512)

    def compute(g):
        gg = plane(g)
        for yy in range(Y):
            for j in range(B // NB):
                h = jnp.dot(tokg[gg], upg[yy, :, rows(j * NB, NB)], preferred_element_type=f32)
                h = jnp.maximum(h, 0.0)
                hid[gg, :, rows(yy * B + j * NB, NB)] = (h * h).astype(bf16)

    def sum_c(gg, f):
        return rcopy(part.at[gg, f, oc], cin.at[gg, f], rc_s.at[0], rc_r.at[gg, f], dev(cc=oc))

    def project(q, g):
        gg = plane(g)

        @pl.loop(0, X)
        def _(xx):
            f = plane(q) * X + xx
            v = jnp.dot(hid[gg], downg[f], preferred_element_type=f32).astype(bf16)
            for cc in range(C):
                part[gg, f, cc] = v[cc * T:(cc + 1) * T]
            sum_c(gg, f).start()

    def sum_z(me, g, f, way, slot):
        to = jnp.where(low, z + way, z - way)
        return rcopy(zout.at[plane(g), f], zin.at[slot, f], rz_s.at[0], rz_r.at[slot, f], dev(zz=to))

    def step(me, g, q):
        gg = plane(g)

        @pl.loop(0, X)
        def _(xx):
            f = plane(q) * X + xx
            sum_c(gg, f).wait_recv()
            acc = part[gg, f, c].astype(f32) + cin[gg, f].astype(f32)
            slots = ([g] if me > 0 and g >= me else []) + ([g and Z] if g <= me else [])
            for slot in slots:
                sum_z(me, g, f, 1, slot).wait_recv()
                acc = acc + zin[slot, f].astype(f32)
            if g == me:
                out[:, rows(f * Dl, Dl)] = acc.astype(bf16)
            else:
                zout[gg, f] = acc.astype(bf16)
                if g < me:
                    sum_z(me, g, f, -1, 0).start()
                else:
                    sum_z(me, g, f, 1, g if me == 0 else (Z - 1 - g) and Z).start()

    def run(me, op, *args):
        k = 0 if op[0] == "u" else 1
        if op == "norm":
            normalize()
        elif op == "uown" or op == "down_own":
            for half in range(2):
                wx(me, k, half).start()
                wy(me, k, half).start()
        elif op == "usend" or op == "dsend":
            wz(args[0], k, args[1]).start()
        elif op == "urel" or op == "drel":
            q, half = args
            wz_recv(q, k, half).wait_recv()
            wx(q, k, half).start()
            wy(q, k, half).start()
        elif op == "udiag" or op == "ddiag":
            q, half = args
            if half == 0:
                wx(q, k, 0, ox).wait_recv()
            else:
                wy(q, k, 1, oy).wait_recv()
            wd(q, k, half).start()
        elif op == "uall" or op == "dall":
            q = args[0]
            rest_recv(q, k).wait_recv()
        elif op == "tsend":
            cut, way = args
            if way == 0:
                tok_c(me, cut).start()
            else:
                tok_z(me, cut, way).start()
        elif op == "trel":
            g, cut = args
            tok_z(g, cut, 1 if g < me else -1).wait_recv()
            if me > 0:
                tok_z(g, cut, 1 if g < me else -1).start()
            tok_c(g, cut).start()
        elif op == "hid":
            ref = tokg.at[plane(args[0]), rows(oc * T, T)]
            rcopy(ref, ref, tc_s.at[0], tc_r.at[plane(args[0])], dev(cc=oc)).wait_recv()
            compute(args[0])
        elif op == "proj":
            project(*args)
        elif op == "sum":
            step(me, *args)

    def sent(ref, sem):
        rcopy(ref, ref, sem.at[0], rc_r.at[0, 0], dev(cc=oc)).wait_send()

    def drain(me):
        sent(upg.at[:, pl.ds(0, (Z - 1) * Dl)], wz_s)
        sent(upg.at[0], wx_s)
        sent(upg.at[0], wy_s)
        sent(upg.at[0], wd_s)
        sent(tokg.at[0, pl.ds(0, T)] if me == 0 else upg.at[:, pl.ds(0, 5 * Dl)], t_s)
        sent(tokg.at[pl.ds(0, 2)], tc_s)
        sent(zout.at[pl.ds(0, Z - 1)], rz_s)
        sent(zout, rc_s)

    for me in range(Z // 2):
        @pl.when(p == me)
        def _(me=me):
            for item in PROGRAM[me]:
                run(me, *item)
            drain(me)


def solution(mesh):
    n_fs, n_tp = mesh.shape["fs"], mesh.shape["tp"]
    X = 2 ** (int(math.log2(n_fs)) // 2)
    Z = n_fs // X
    C = 2
    Y = n_tp // C
    placed = (P(("fs", "tp"), None), P(), P("fs", "tp"), P("tp", "fs"))

    def on_device(tokens, norm_gain, up_weight, down_weight):
        T, D = tokens.shape
        Dl, FFl = up_weight.shape
        B = FFl // Z
        if X != 2 or Y != 2 or Z != 4 or Z * X != n_fs or Dl % 256 or B % 256 or T % (16 * CUTS):
            return plain(tokens, norm_gain, up_weight, down_weight)
        F = Z * X
        dma = pltpu.SemaphoreType.DMA
        vm = pl.BlockSpec(memory_space=pltpu.VMEM)
        hbm = pl.BlockSpec(memory_space=pltpu.HBM)
        return pl.pallas_call(
            functools.partial(kernel, Z, X, Y, C),
            out_shape=jax.ShapeDtypeStruct((T, D), bf16),
            in_specs=[hbm, vm, hbm, hbm],
            out_specs=vm,
            scratch_shapes=[
                pltpu.VMEM((T, D), bf16),
                pltpu.VMEM((Dl, FFl), bf16),
                pltpu.VMEM((FFl, Dl), bf16),
                pltpu.VMEM((Z, C * T, D), bf16),
                pltpu.VMEM((Y, D, B), bf16),
                pltpu.VMEM((F, Y * B, Dl), bf16),
                pltpu.VMEM((Z, C * T, Y * B), bf16),
                pltpu.VMEM((Z, F, C, T, Dl), bf16),
                pltpu.VMEM((Z, F, T, Dl), bf16),
                pltpu.VMEM((Z + 1, F, T, Dl), bf16),
                pltpu.VMEM((Z, F, T, Dl), bf16),
                dma((5,)),
                *[dma((1,)) for _ in range(8)],
                dma((2, Z, 2)), dma((2, Z)), dma((2, Z)), dma((2, Z)),
                dma((Z, CUTS)), dma((Z,)), dma((Z, F)), dma((Z + 1, F)),
            ],
            compiler_params=pltpu.CompilerParams(
                collective_id=0, has_side_effects=True, vmem_limit_bytes=53 * 2**20),
        )(tokens, norm_gain.reshape(1, D), up_weight, down_weight)

    return jax.shard_map(
        on_device, mesh=mesh, in_specs=placed, out_specs=P(("fs", "tp"), None), check_vma=False)
```

```python
import functools
import math

import jax
import jax.numpy as jnp
from jax import lax
from jax.experimental import pallas as pl
from jax.experimental.pallas import tpu as pltpu
from jax.sharding import PartitionSpec as P

epsilon = 1e-06
MESH = pl.DeviceIdType.MESH
CUTS = 4
f32, bf16 = jnp.float32, jnp.bfloat16


def plain(tokens, norm_gain, up_weight, down_weight):
    values = tokens.astype(f32)
    mean_square = jnp.mean(values * values, axis=-1, keepdims=True)
    normed = (values * lax.rsqrt(mean_square + epsilon) * norm_gain).astype(bf16)
    up_whole = lax.all_gather(up_weight, "fs", axis=0, tiled=True)
    rows = lax.all_gather(normed, "tp", axis=0, tiled=True)
    preact = jnp.dot(rows, up_whole, preferred_element_type=f32)
    hidden = jnp.square(jnp.maximum(preact, 0.0)).astype(bf16)
    down_whole = lax.all_gather(down_weight, "fs", axis=1, tiled=True)
    partial_value = jnp.dot(hidden, down_whole, preferred_element_type=f32).astype(bf16)
    return lax.psum_scatter(partial_value, "tp", scatter_dimension=0, tiled=True)


PROGRAM = {
    0: [
        ("uown",), ("norm",), ("usend", 2, 1), ("usend", 1, 0), ("urel", 1, 1), ("dsend", 1, 1), ("usend", 3, 1),
        ("tsend", 3, 1), ("down_own",), ("usend", 1, 1), ("usend", 3, 0), ("urel", 2, 0), ("urel", 3, 1),
        ("urel", 1, 0), ("dsend", 2, 0), ("tsend", 1, 1), ("udiag", 0, 1), ("udiag", 0, 0), ("usend", 2, 0),
        ("dsend", 3, 1), ("tsend", 2, 1), ("urel", 3, 0), ("udiag", 2, 0), ("udiag", 3, 1), ("ddiag", 0, 0),
        ("tsend", 0, 0), ("urel", 2, 1), ("udiag", 1, 1), ("dsend", 1, 0), ("drel", 1, 1), ("udiag", 1, 0),
        ("tsend", 1, 0), ("tsend", 0, 1), ("trel", 1, 2), ("udiag", 3, 0), ("trel", 1, 1), ("udiag", 2, 1),
        ("dsend", 3, 0), ("ddiag", 0, 1), ("drel", 1, 0), ("tsend", 2, 0), ("tsend", 3, 0), ("ddiag", 1, 1),
        ("dsend", 2, 1), ("uall", 1), ("uall", 3), ("trel", 1, 3), ("trel", 2, 2), ("uall", 2), ("trel", 1, 0),
        ("drel", 3, 0), ("uall", 0), ("trel", 3, 3), ("dall", 0), ("ddiag", 1, 0), ("hid", 1), ("drel", 3, 1),
        ("proj", 0, 1), ("dall", 1), ("trel", 3, 0), ("ddiag", 3, 0), ("ddiag", 3, 1), ("trel", 2, 3), ("sum", 1, 0),
        ("proj", 1, 1), ("trel", 3, 1), ("trel", 3, 2), ("sum", 1, 1), ("hid", 3), ("drel", 2, 0), ("dall", 3),
        ("proj", 0, 3), ("proj", 1, 3), ("sum", 3, 0), ("drel", 2, 1), ("proj", 3, 3), ("hid", 0), ("proj", 1, 0),
        ("trel", 2, 1), ("ddiag", 2, 0), ("sum", 3, 3), ("sum", 3, 1), ("trel", 2, 0), ("ddiag", 2, 1), ("hid", 2),
        ("proj", 3, 2), ("proj", 0, 2), ("sum", 2, 3), ("dall", 2), ("proj", 2, 3), ("sum", 3, 2), ("sum", 2, 0),
        ("proj", 1, 2), ("proj", 3, 1), ("proj", 2, 1), ("proj", 2, 2), ("proj", 0, 0), ("sum", 2, 1), ("sum", 2, 2),
        ("sum", 1, 2), ("sum", 1, 3), ("proj", 3, 0), ("sum", 0, 3), ("proj", 2, 0), ("sum", 0, 2), ("sum", 0, 1),
        ("sum", 0, 0),
    ],
    1: [
        ("usend", 0, 1), ("uown",), ("usend", 0, 0), ("usend", 2, 1), ("norm",), ("usend", 3, 0), ("tsend", 3, -1),
        ("down_own",), ("tsend", 2, -1), ("usend", 3, 1), ("usend", 2, 0), ("urel", 2, 1), ("dsend", 0, 0),
        ("drel", 0, 1), ("tsend", 1, -1), ("tsend", 3, 0), ("tsend", 2, 1), ("trel", 0, 3), ("dsend", 0, 1),
        ("urel", 2, 0), ("udiag", 1, 1), ("drel", 3, 0), ("trel", 0, 1), ("urel", 0, 1), ("trel", 2, 2),
        ("udiag", 1, 0), ("urel", 3, 1), ("urel", 0, 0), ("tsend", 3, 1), ("tsend", 0, 0), ("urel", 3, 0),
        ("trel", 3, 3), ("trel", 0, 2), ("udiag", 2, 1), ("tsend", 0, -1), ("ddiag", 1, 0), ("trel", 3, 1),
        ("trel", 2, 3), ("trel", 0, 0), ("tsend", 0, 1), ("udiag", 0, 1), ("tsend", 1, 1), ("udiag", 3, 1),
        ("udiag", 3, 0), ("drel", 3, 1), ("udiag", 2, 0), ("udiag", 0, 0), ("tsend", 1, 0), ("uall", 1),
        ("dsend", 3, 0), ("dsend", 3, 1), ("uall", 3), ("trel", 3, 2), ("drel", 0, 0), ("trel", 3, 0),
        ("ddiag", 1, 1), ("ddiag", 3, 0), ("uall", 0), ("ddiag", 3, 1), ("tsend", 2, 0), ("dsend", 2, 0),
        ("dsend", 2, 1), ("uall", 2), ("hid", 1), ("dall", 1), ("trel", 2, 1), ("trel", 2, 0), ("ddiag", 0, 1),
        ("ddiag", 0, 0), ("hid", 3), ("hid", 2), ("proj", 1, 3), ("dall", 0), ("dall", 3), ("drel", 2, 0),
        ("proj", 0, 3), ("proj", 0, 2), ("proj", 1, 1), ("drel", 2, 1), ("sum", 3, 0), ("proj", 3, 3), ("hid", 0),
        ("proj", 0, 0), ("proj", 1, 2), ("sum", 3, 3), ("proj", 3, 0), ("proj", 0, 1), ("ddiag", 2, 0),
        ("ddiag", 2, 1), ("proj", 3, 1), ("proj", 3, 2), ("sum", 0, 3), ("sum", 3, 1), ("sum", 2, 3), ("sum", 0, 0),
        ("dall", 2), ("proj", 1, 0), ("proj", 2, 3), ("sum", 3, 2), ("sum", 2, 0), ("proj", 2, 2), ("proj", 2, 1),
        ("sum", 0, 1), ("proj", 2, 0), ("sum", 1, 0), ("sum", 2, 1), ("sum", 0, 2), ("sum", 2, 2), ("sum", 1, 2),
        ("sum", 1, 1), ("sum", 1, 3),
    ],
}


def kernel(Z, X, Y, C, tok, gain, up, down, out,
           tokb, gainb, upb, downb, tokg, upg, downg, hid, part, cin, zin, zout,
           in_s, wz_s, wx_s, wy_s, wd_s, t_s, tc_s, rc_s, rz_s,
           wz_r, wx_r, wy_r, all_r, t_r, tc_r, rc_r, rz_r):
    T, D = tok.shape
    F = Z * X
    Dl = up.shape[0]
    B = upg.shape[2]
    fs, tp = lax.axis_index("fs"), lax.axis_index("tp")
    z, x = fs // X, fs % X
    y, c = tp // C, tp % C
    ox, oy, oc = X - 1 - x, Y - 1 - y, C - 1 - c
    low = z < Z // 2
    p = jnp.where(low, z, Z - 1 - z)

    def plane(q):
        return jnp.where(low, q, Z - 1 - q)

    def dev(zz=z, xx=x, yy=y, cc=c):
        return {"fs": zz * X + xx, "tp": yy * C + cc}

    def rcopy(src, dst, ss, rs, device):
        return pltpu.make_async_remote_copy(
            src_ref=src, dst_ref=dst, send_sem=ss, recv_sem=rs,
            device_id=device, device_id_type=MESH)

    def rows(start, size):
        return pl.ds(pl.multiple_of(start, size), size)

    barrier = pltpu.get_barrier_semaphore()
    peers = [dev(zz=(z + k) % Z) for k in range(1, Z)]
    peers += [dev(xx=ox), dev(yy=oy), dev(cc=oc)]
    for peer in peers:
        pl.semaphore_signal(barrier, inc=1, device_id=peer, device_id_type=MESH)

    loads = [
        pltpu.make_async_copy(up, upb, in_s.at[0]),
        pltpu.make_async_copy(up.at[:, rows(z * B, B)], upg.at[y, rows(fs * Dl, Dl)], in_s.at[1]),
        pltpu.make_async_copy(tok, tokb, in_s.at[2]),
        pltpu.make_async_copy(gain, gainb, in_s.at[5]),
        pltpu.make_async_copy(down, downb, in_s.at[3]),
        pltpu.make_async_copy(down.at[rows(z * B, B)], downg.at[fs, rows(y * B, B)], in_s.at[4]),
    ]
    for load in loads[:4]:
        load.start()
    loads[0].wait()
    for load in loads[4:]:
        load.start()
    loads[1].wait()
    pl.semaphore_wait(barrier, len(peers))

    def normalize():
        loads[2].wait()
        loads[3].wait()
        RB = 32

        @pl.loop(0, T // RB)
        def _(i):
            v = tokb[rows(i * RB, RB), :].astype(f32)
            ms = jnp.mean(v * v, axis=-1, keepdims=True)
            tokg[z, rows(c * T + i * RB, RB), :] = (v * lax.rsqrt(ms + epsilon) * gainb[...]).astype(bf16)

        loads[4].wait()
        loads[5].wait()

    def piece(zz, xx, yy, k, half):
        f = zz * X + xx
        if k == 0:
            return upg.at[yy, rows(f * Dl + half * (Dl // 2), Dl // 2)]
        return downg.at[f, rows(yy * B + half * (B // 2), B // 2)]

    def own_piece(zz, k, half):
        if k == 0:
            return upb.at[rows(half * (Dl // 2), Dl // 2), rows(zz * B, B)]
        return downb.at[rows(zz * B + half * (B // 2), B // 2)]

    def wz(q, k, half):
        zz = plane(q)
        return rcopy(own_piece(zz, k, half), piece(z, x, y, k, half),
                     wz_s.at[0], wz_r.at[k, z, half], dev(zz=zz))

    def wz_recv(q, k, half):
        zz = plane(q)
        ref = piece(zz, x, y, k, half)
        return rcopy(ref, ref, wz_s.at[0], wz_r.at[k, zz, half], dev(zz=zz))

    def wx(q, k, half, xx=x):
        zz = plane(q)
        ref = piece(zz, xx, y, k, half)
        rs = wx_r.at[k, zz] if half == 0 else all_r.at[k, zz]
        return rcopy(ref, ref, wx_s.at[0], rs, dev(xx=ox))

    def wy(q, k, half, yy=y):
        zz = plane(q)
        ref = piece(zz, x, yy, k, half)
        rs = wy_r.at[k, zz] if half == 1 else all_r.at[k, zz]
        return rcopy(ref, ref, wy_s.at[0], rs, dev(yy=oy))

    def wd(q, k, half):
        zz = plane(q)
        ref = piece(zz, ox, y, k, 0) if half == 0 else piece(zz, x, oy, k, 1)
        to = dev(yy=oy) if half == 0 else dev(xx=ox)
        return rcopy(ref, ref, wd_s.at[0], all_r.at[k, zz], to)

    def rest_recv(q, k):
        zz = plane(q)
        ref = upg.at[y, pl.ds(0, 2 * Dl)] if k == 0 else downg.at[zz * X]
        return rcopy(ref, ref, wd_s.at[0], all_r.at[k, zz], dev(yy=oy))

    TC = T // CUTS

    def tok_z(g, cut, way):
        gg = plane(g)
        ref = tokg.at[gg, rows(c * T + cut * TC, TC)]
        to = jnp.where(low, z + way, z - way)
        return rcopy(ref, ref, t_s.at[0], t_r.at[gg, cut], dev(zz=to))

    def tok_c(g, cut, cc=c):
        gg = plane(g)
        ref = tokg.at[gg, rows(cc * T + cut * TC, TC)]
        return rcopy(ref, ref, tc_s.at[0], tc_r.at[gg], dev(cc=oc))

    NB = min(B, 512)

    def compute(g):
        gg = plane(g)
        for yy in range(Y):
            for j in range(B // NB):
                h = jnp.dot(tokg[gg], upg[yy, :, rows(j * NB, NB)], preferred_element_type=f32)
                h = jnp.maximum(h, 0.0)
                hid[gg, :, rows(yy * B + j * NB, NB)] = (h * h).astype(bf16)

    def sum_c(g, q, f):
        gg, zz = plane(g), plane(q)
        return rcopy(part.at[gg, f, oc], cin.at[gg, f], rc_s.at[0], rc_r.at[gg, zz], dev(cc=oc))

    def sum_c_recv(g, q):
        gg, zz = plane(g), plane(q)
        ref = cin.at[gg, pl.ds(zz * X, X)]
        return rcopy(ref, ref, rc_s.at[0], rc_r.at[gg, zz], dev(cc=oc))

    def project(q, g):
        gg = plane(g)

        @pl.loop(0, X)
        def _(xx):
            f = plane(q) * X + xx
            v = jnp.dot(hid[gg], downg[f], preferred_element_type=f32).astype(bf16)
            for cc in range(C):
                part[gg, f, cc] = v[cc * T:(cc + 1) * T]
            sum_c(g, q, f).start()

    def sum_z(me, g, f, way, slot):
        to = jnp.where(low, z + way, z - way)
        return rcopy(zout.at[plane(g), f], zin.at[slot, f], rz_s.at[0], rz_r.at[slot, f], dev(zz=to))

    def step(me, g, q):
        gg = plane(g)
        sum_c_recv(g, q).wait_recv()

        @pl.loop(0, X)
        def _(xx):
            f = plane(q) * X + xx
            acc = part[gg, f, c].astype(f32) + cin[gg, f].astype(f32)
            slots = ([g] if me > 0 and g >= me else []) + ([g and Z] if g <= me else [])
            for slot in slots:
                sum_z(me, g, f, 1, slot).wait_recv()
                acc = acc + zin[slot, f].astype(f32)
            if g == me:
                out[:, rows(f * Dl, Dl)] = acc.astype(bf16)
            else:
                zout[gg, f] = acc.astype(bf16)
                if g < me:
                    sum_z(me, g, f, -1, 0).start()
                else:
                    sum_z(me, g, f, 1, g if me == 0 else (Z - 1 - g) and Z).start()

    def run(me, op, *args):
        k = 0 if op[0] == "u" else 1
        if op == "norm":
            normalize()
        elif op == "uown" or op == "down_own":
            for half in range(2):
                wx(me, k, half).start()
                wy(me, k, half).start()
        elif op == "usend" or op == "dsend":
            wz(args[0], k, args[1]).start()
        elif op == "urel" or op == "drel":
            q, half = args
            wz_recv(q, k, half).wait_recv()
            wx(q, k, half).start()
            wy(q, k, half).start()
        elif op == "udiag" or op == "ddiag":
            q, half = args
            if half == 0:
                wx(q, k, 0, ox).wait_recv()
            else:
                wy(q, k, 1, oy).wait_recv()
            wd(q, k, half).start()
        elif op == "uall" or op == "dall":
            q = args[0]
            rest_recv(q, k).wait_recv()
        elif op == "tsend":
            cut, way = args
            if way == 0:
                tok_c(me, cut).start()
            else:
                tok_z(me, cut, way).start()
        elif op == "trel":
            g, cut = args
            tok_z(g, cut, 1 if g < me else -1).wait_recv()
            if me > 0:
                tok_z(g, cut, 1 if g < me else -1).start()
            tok_c(g, cut).start()
        elif op == "hid":
            ref = tokg.at[plane(args[0]), rows(oc * T, T)]
            rcopy(ref, ref, tc_s.at[0], tc_r.at[plane(args[0])], dev(cc=oc)).wait_recv()
            compute(args[0])
        elif op == "proj":
            project(*args)
        elif op == "sum":
            step(me, *args)

    def sent(ref, sem):
        rcopy(ref, ref, sem.at[0], rc_r.at[0, 0], dev(cc=oc)).wait_send()

    def drain(me):
        sent(upg.at[:, pl.ds(0, (Z - 1) * Dl)], wz_s)
        sent(upg.at[0], wx_s)
        sent(upg.at[0], wy_s)
        sent(upg.at[0], wd_s)
        sent(tokg.at[0, pl.ds(0, T)] if me == 0 else upg.at[:, pl.ds(0, 5 * Dl)], t_s)
        sent(tokg.at[pl.ds(0, 2)], tc_s)
        sent(zout.at[pl.ds(0, Z - 1)], rz_s)
        sent(zout, rc_s)

    for me in range(Z // 2):
        @pl.when(p == me)
        def _(me=me):
            for item in PROGRAM[me]:
                run(me, *item)
            drain(me)


def solution(mesh):
    n_fs, n_tp = mesh.shape["fs"], mesh.shape["tp"]
    X = 2 ** (int(math.log2(n_fs)) // 2)
    Z = n_fs // X
    C = 2
    Y = n_tp // C
    placed = (P(("fs", "tp"), None), P(), P("fs", "tp"), P("tp", "fs"))

    def on_device(tokens, norm_gain, up_weight, down_weight):
        T, D = tokens.shape
        Dl, FFl = up_weight.shape
        B = FFl // Z
        if X != 2 or Y != 2 or Z != 4 or Z * X != n_fs or Dl % 256 or B % 256 or T % (16 * CUTS):
            return plain(tokens, norm_gain, up_weight, down_weight)
        F = Z * X
        dma = pltpu.SemaphoreType.DMA
        vm = pl.BlockSpec(memory_space=pltpu.VMEM)
        hbm = pl.BlockSpec(memory_space=pltpu.HBM)
        return pl.pallas_call(
            functools.partial(kernel, Z, X, Y, C),
            out_shape=jax.ShapeDtypeStruct((T, D), bf16),
            in_specs=[hbm] * 4,
            out_specs=vm,
            scratch_shapes=[
                pltpu.VMEM((T, D), bf16),
                pltpu.VMEM((1, D), f32),
                pltpu.VMEM((Dl, FFl), bf16),
                pltpu.VMEM((FFl, Dl), bf16),
                pltpu.VMEM((Z, C * T, D), bf16),
                pltpu.VMEM((Y, D, B), bf16),
                pltpu.VMEM((F, Y * B, Dl), bf16),
                pltpu.VMEM((Z, C * T, Y * B), bf16),
                pltpu.VMEM((Z, F, C, T, Dl), bf16),
                pltpu.VMEM((Z, F, T, Dl), bf16),
                pltpu.VMEM((Z + 1, F, T, Dl), bf16),
                pltpu.VMEM((Z, F, T, Dl), bf16),
                dma((6,)),
                *[dma((1,)) for _ in range(8)],
                dma((2, Z, 2)), dma((2, Z)), dma((2, Z)), dma((2, Z)),
                dma((Z, CUTS)), dma((Z,)), dma((Z, Z)), dma((Z + 1, F)),
            ],
            compiler_params=pltpu.CompilerParams(
                collective_id=0, has_side_effects=True, vmem_limit_bytes=48 * 2**20),
        )(*[pltpu.with_memory_space_constraint(v, pltpu.HBM)
            for v in (tokens, norm_gain.reshape(1, D), up_weight, down_weight)])

    return jax.shard_map(
        on_device, mesh=mesh, in_specs=placed, out_specs=P(("fs", "tp"), None), check_vma=False)
```

```python
import functools
import math

import jax
import jax.numpy as jnp
from jax import lax
from jax.experimental import pallas as pl
from jax.experimental.pallas import tpu as pltpu
from jax.sharding import PartitionSpec as P

epsilon = 1e-06
MESH = pl.DeviceIdType.MESH
CUTS = 4
f32, bf16 = jnp.float32, jnp.bfloat16


def plain(tokens, norm_gain, up_weight, down_weight):
    values = tokens.astype(f32)
    mean_square = jnp.mean(values * values, axis=-1, keepdims=True)
    normed = (values * lax.rsqrt(mean_square + epsilon) * norm_gain).astype(bf16)
    up_whole = lax.all_gather(up_weight, "fs", axis=0, tiled=True)
    rows = lax.all_gather(normed, "tp", axis=0, tiled=True)
    preact = jnp.dot(rows, up_whole, preferred_element_type=f32)
    hidden = jnp.square(jnp.maximum(preact, 0.0)).astype(bf16)
    down_whole = lax.all_gather(down_weight, "fs", axis=1, tiled=True)
    partial_value = jnp.dot(hidden, down_whole, preferred_element_type=f32).astype(bf16)
    return lax.psum_scatter(partial_value, "tp", scatter_dimension=0, tiled=True)


PROGRAM = {
    0: [
        ("uown",), ("usend", 3, 0), ("norm",), ("usend", 1, 1), ("dsend", 2, 0), ("tsend", 1, 1), ("down_own",),
        ("tsend", 0, 1), ("dsend", 1, 0), ("udiag", 0, 1), ("urel", 1, 1), ("drel", 1, 1), ("udiag", 1, 1),
        ("udiag", 0, 0), ("tsend", 2, 1), ("usend", 3, 1), ("ddiag", 0, 0), ("tsend", 2, 0), ("urel", 2, 1),
        ("trel", 1, 1), ("usend", 2, 0), ("urel", 3, 0), ("tsend", 3, 1), ("urel", 2, 0), ("drel", 1, 0), ("uall", 0),
        ("trel", 1, 2), ("urel", 3, 1), ("dsend", 1, 1), ("trel", 1, 0), ("usend", 1, 0), ("urel", 1, 0),
        ("ddiag", 0, 1), ("ddiag", 1, 1), ("trel", 3, 0), ("ddiag", 1, 0), ("usend", 2, 1), ("udiag", 1, 0),
        ("udiag", 3, 1), ("dsend", 2, 1), ("trel", 3, 2), ("dsend", 3, 0), ("tsend", 0, 0), ("udiag", 3, 0),
        ("uall", 1), ("udiag", 2, 1), ("dsend", 3, 1), ("udiag", 2, 0), ("trel", 1, 3), ("dall", 0), ("drel", 3, 1),
        ("drel", 3, 0), ("trel", 3, 1), ("trel", 3, 3), ("uall", 2), ("dall", 1), ("tsend", 3, 0), ("uall", 3),
        ("hid", 1), ("proj", 0, 1), ("hid", 3), ("proj", 1, 3), ("tsend", 1, 0), ("sum", 1, 0), ("proj", 0, 3),
        ("ddiag", 3, 0), ("ddiag", 3, 1), ("sum", 3, 1), ("trel", 2, 3), ("hid", 0), ("proj", 0, 0), ("dall", 3),
        ("sum", 3, 0), ("proj", 3, 3), ("trel", 2, 1), ("proj", 3, 1), ("trel", 2, 0), ("sum", 3, 3), ("trel", 2, 2),
        ("drel", 2, 1), ("sum", 1, 3), ("hid", 2), ("proj", 3, 2), ("proj", 1, 1), ("drel", 2, 0), ("proj", 0, 2),
        ("sum", 2, 3), ("proj", 1, 2), ("sum", 2, 0), ("ddiag", 2, 0), ("ddiag", 2, 1), ("sum", 2, 1), ("dall", 2),
        ("proj", 2, 3), ("sum", 3, 2), ("proj", 2, 2), ("sum", 2, 2), ("proj", 2, 1), ("proj", 3, 0), ("sum", 0, 3),
        ("sum", 1, 2), ("proj", 1, 0), ("sum", 1, 1), ("sum", 0, 0), ("proj", 2, 0), ("sum", 0, 1), ("sum", 0, 2),
    ],
    1: [
        ("uown",), ("usend", 2, 0), ("norm",), ("usend", 0, 1), ("dsend", 0, 1), ("tsend", 1, -1), ("usend", 2, 1),
        ("down_own",), ("usend", 3, 0), ("tsend", 0, -1), ("ddiag", 1, 0), ("urel", 2, 1), ("drel", 3, 0),
        ("urel", 0, 1), ("tsend", 1, 0), ("udiag", 1, 1), ("usend", 3, 1), ("trel", 0, 0), ("tsend", 2, -1),
        ("dsend", 0, 0), ("ddiag", 3, 0), ("trel", 0, 2), ("urel", 2, 0), ("tsend", 3, 0), ("usend", 0, 0),
        ("tsend", 0, 0), ("trel", 0, 1), ("trel", 3, 0), ("ddiag", 1, 1), ("tsend", 2, 1), ("udiag", 1, 0),
        ("trel", 0, 3), ("urel", 3, 0), ("trel", 3, 1), ("drel", 0, 1), ("tsend", 2, 0), ("tsend", 3, -1),
        ("udiag", 3, 0), ("tsend", 3, 1), ("urel", 0, 0), ("trel", 3, 2), ("trel", 3, 3), ("urel", 3, 1),
        ("tsend", 0, 1), ("tsend", 1, 1), ("udiag", 2, 1), ("uall", 1), ("drel", 3, 1), ("udiag", 3, 1),
        ("trel", 2, 2), ("drel", 0, 0), ("udiag", 2, 0), ("udiag", 0, 1), ("dsend", 2, 0), ("trel", 2, 3),
        ("trel", 2, 0), ("ddiag", 0, 1), ("dsend", 2, 1), ("udiag", 0, 0), ("dsend", 3, 1), ("trel", 2, 1),
        ("ddiag", 0, 0), ("uall", 0), ("uall", 3), ("dall", 1), ("uall", 2), ("hid", 3), ("proj", 1, 3), ("dall", 0),
        ("ddiag", 3, 1), ("drel", 2, 0), ("dsend", 3, 0), ("proj", 0, 3), ("hid", 1), ("drel", 2, 1), ("dall", 3),
        ("sum", 3, 0), ("proj", 3, 1), ("proj", 3, 3), ("hid", 0), ("ddiag", 2, 1), ("proj", 1, 0), ("proj", 3, 0),
        ("ddiag", 2, 0), ("hid", 2), ("proj", 3, 2), ("sum", 3, 3), ("sum", 3, 1), ("proj", 0, 2), ("sum", 0, 3),
        ("sum", 2, 3), ("dall", 2), ("proj", 2, 1), ("proj", 0, 1), ("proj", 2, 0), ("proj", 2, 2), ("proj", 0, 0),
        ("proj", 1, 1), ("sum", 2, 0), ("sum", 0, 0), ("sum", 0, 2), ("proj", 2, 3), ("sum", 1, 0), ("sum", 3, 2),
        ("sum", 1, 3), ("proj", 1, 2), ("sum", 2, 1), ("sum", 2, 2), ("sum", 0, 1), ("sum", 1, 2), ("sum", 1, 1),
    ],
}


def kernel(Z, X, Y, C, tok, gain, up, down, out,
           tokb, gainb, upb, downb, tokg, upg, downg, hid, part, cin, zin, zout,
           in_s, wz_s, wx_s, wy_s, wd_s, t_s, tc_s, rc_s, rz_s,
           wz_r, wx_r, wy_r, all_r, t_r, tc_r, rc_r, rz_r):
    T, D = tok.shape
    F = Z * X
    Dl = up.shape[0]
    B = upg.shape[2]
    fs, tp = lax.axis_index("fs"), lax.axis_index("tp")
    z, x = fs // X, fs % X
    y, c = tp // C, tp % C
    ox, oy, oc = X - 1 - x, Y - 1 - y, C - 1 - c
    low = z < Z // 2
    p = jnp.where(low, z, Z - 1 - z)

    def plane(q):
        return jnp.where(low, q, Z - 1 - q)

    def dev(zz=z, xx=x, yy=y, cc=c):
        return {"fs": zz * X + xx, "tp": yy * C + cc}

    def rcopy(src, dst, ss, rs, device):
        return pltpu.make_async_remote_copy(
            src_ref=src, dst_ref=dst, send_sem=ss, recv_sem=rs,
            device_id=device, device_id_type=MESH)

    def rows(start, size):
        return pl.ds(pl.multiple_of(start, size), size)

    barrier = pltpu.get_barrier_semaphore()
    peers = [dev(zz=(z + k) % Z) for k in range(1, Z)]
    peers += [dev(xx=ox), dev(yy=oy), dev(cc=oc)]
    for peer in peers:
        pl.semaphore_signal(barrier, inc=1, device_id=peer, device_id_type=MESH)

    loads = [
        pltpu.make_async_copy(up, upb, in_s.at[0]),
        pltpu.make_async_copy(up.at[:, rows(z * B, B)], upg.at[y, rows(fs * Dl, Dl)], in_s.at[1]),
        pltpu.make_async_copy(tok, tokb, in_s.at[2]),
        pltpu.make_async_copy(gain, gainb, in_s.at[5]),
        pltpu.make_async_copy(down, downb, in_s.at[3]),
        pltpu.make_async_copy(down.at[rows(z * B, B)], downg.at[z, rows(y * B, B), rows(x * Dl, Dl)], in_s.at[4]),
    ]
    for load in loads[:4]:
        load.start()
    loads[0].wait()
    for load in loads[4:]:
        load.start()
    loads[1].wait()
    pl.semaphore_wait(barrier, len(peers))

    def normalize():
        loads[2].wait()
        loads[3].wait()
        RB = 32

        @pl.loop(0, T // RB)
        def _(i):
            v = tokb[rows(i * RB, RB), :].astype(f32)
            ms = jnp.mean(v * v, axis=-1, keepdims=True)
            tokg[z, rows(c * T + i * RB, RB), :] = (v * lax.rsqrt(ms + epsilon) * gainb[...]).astype(bf16)

        loads[4].wait()
        loads[5].wait()

    def piece(zz, xx, yy, k, half):
        f = zz * X + xx
        if k == 0:
            return upg.at[yy, rows(f * Dl + half * (Dl // 2), Dl // 2)]
        return downg.at[zz, rows(yy * B + half * (B // 2), B // 2), rows(xx * Dl, Dl)]

    def own_piece(zz, k, half):
        if k == 0:
            return upb.at[rows(half * (Dl // 2), Dl // 2), rows(zz * B, B)]
        return downb.at[rows(zz * B + half * (B // 2), B // 2)]

    def wz(q, k, half):
        zz = plane(q)
        return rcopy(own_piece(zz, k, half), piece(z, x, y, k, half),
                     wz_s.at[0], wz_r.at[k, z, half], dev(zz=zz))

    def wz_recv(q, k, half):
        zz = plane(q)
        ref = piece(zz, x, y, k, half)
        return rcopy(ref, ref, wz_s.at[0], wz_r.at[k, zz, half], dev(zz=zz))

    def wx(q, k, half, xx=x):
        zz = plane(q)
        ref = piece(zz, xx, y, k, half)
        rs = wx_r.at[k, zz] if half == 0 else all_r.at[k, zz]
        return rcopy(ref, ref, wx_s.at[0], rs, dev(xx=ox))

    def wy(q, k, half, yy=y):
        zz = plane(q)
        ref = piece(zz, x, yy, k, half)
        rs = wy_r.at[k, zz] if half == 1 else all_r.at[k, zz]
        return rcopy(ref, ref, wy_s.at[0], rs, dev(yy=oy))

    def wd(q, k, half):
        zz = plane(q)
        ref = piece(zz, ox, y, k, 0) if half == 0 else piece(zz, x, oy, k, 1)
        to = dev(yy=oy) if half == 0 else dev(xx=ox)
        return rcopy(ref, ref, wd_s.at[0], all_r.at[k, zz], to)

    def rest_recv(q, k):
        zz = plane(q)
        ref = upg.at[y, pl.ds(0, 2 * Dl)] if k == 0 else downg.at[zz, :, pl.ds(0, Dl)]
        return rcopy(ref, ref, wd_s.at[0], all_r.at[k, zz], dev(yy=oy))

    TC = T // CUTS

    def tok_z(g, cut, way):
        gg = plane(g)
        ref = tokg.at[gg, rows(c * T + cut * TC, TC)]
        to = jnp.where(low, z + way, z - way)
        return rcopy(ref, ref, t_s.at[0], t_r.at[gg, cut], dev(zz=to))

    def tok_c(g, cut, cc=c):
        gg = plane(g)
        ref = tokg.at[gg, rows(cc * T + cut * TC, TC)]
        return rcopy(ref, ref, tc_s.at[0], tc_r.at[gg], dev(cc=oc))

    NB = min(B, 512)

    def compute(g):
        gg = plane(g)
        for yy in range(Y):
            for j in range(B // NB):
                h = jnp.dot(tokg[gg], upg[yy, :, rows(j * NB, NB)], preferred_element_type=f32)
                h = jnp.maximum(h, 0.0)
                hid[gg, :, rows(yy * B + j * NB, NB)] = (h * h).astype(bf16)

    def sum_c(g, q, f):
        gg, zz = plane(g), plane(q)
        return rcopy(part.at[gg, f, oc], cin.at[gg, f], rc_s.at[0], rc_r.at[gg, zz], dev(cc=oc))

    def sum_c_recv(g, q):
        gg, zz = plane(g), plane(q)
        ref = cin.at[gg, pl.ds(zz * X, X)]
        return rcopy(ref, ref, rc_s.at[0], rc_r.at[gg, zz], dev(cc=oc))

    def project(q, g):
        gg, zz = plane(g), plane(q)
        v = jnp.dot(hid[gg], downg[zz], preferred_element_type=f32).astype(bf16)
        for xx in range(X):
            for cc in range(C):
                part[gg, zz * X + xx, cc] = v[cc * T:(cc + 1) * T, xx * Dl:(xx + 1) * Dl]
            sum_c(g, q, zz * X + xx).start()

    def sum_z(me, g, f, way, slot):
        to = jnp.where(low, z + way, z - way)
        return rcopy(zout.at[plane(g), f], zin.at[slot, f], rz_s.at[0], rz_r.at[slot, f], dev(zz=to))

    def step(me, g, q):
        gg = plane(g)
        sum_c_recv(g, q).wait_recv()

        @pl.loop(0, X)
        def _(xx):
            f = plane(q) * X + xx
            acc = part[gg, f, c].astype(f32) + cin[gg, f].astype(f32)
            slots = ([g] if me > 0 and g >= me else []) + ([g and Z] if g <= me else [])
            for slot in slots:
                sum_z(me, g, f, 1, slot).wait_recv()
                acc = acc + zin[slot, f].astype(f32)
            if g == me:
                out[:, rows(f * Dl, Dl)] = acc.astype(bf16)
            else:
                zout[gg, f] = acc.astype(bf16)
                if g < me:
                    sum_z(me, g, f, -1, 0).start()
                else:
                    sum_z(me, g, f, 1, g if me == 0 else (Z - 1 - g) and Z).start()

    def run(me, op, *args):
        k = 0 if op[0] == "u" else 1
        if op == "norm":
            normalize()
        elif op == "uown" or op == "down_own":
            for half in range(2):
                wx(me, k, half).start()
                wy(me, k, half).start()
        elif op == "usend" or op == "dsend":
            wz(args[0], k, args[1]).start()
        elif op == "urel" or op == "drel":
            q, half = args
            wz_recv(q, k, half).wait_recv()
            wx(q, k, half).start()
            wy(q, k, half).start()
        elif op == "udiag" or op == "ddiag":
            q, half = args
            if half == 0:
                wx(q, k, 0, ox).wait_recv()
            else:
                wy(q, k, 1, oy).wait_recv()
            wd(q, k, half).start()
        elif op == "uall" or op == "dall":
            q = args[0]
            rest_recv(q, k).wait_recv()
        elif op == "tsend":
            cut, way = args
            if way == 0:
                tok_c(me, cut).start()
            else:
                tok_z(me, cut, way).start()
        elif op == "trel":
            g, cut = args
            tok_z(g, cut, 1 if g < me else -1).wait_recv()
            if me > 0:
                tok_z(g, cut, 1 if g < me else -1).start()
            tok_c(g, cut).start()
        elif op == "hid":
            ref = tokg.at[plane(args[0]), rows(oc * T, T)]
            rcopy(ref, ref, tc_s.at[0], tc_r.at[plane(args[0])], dev(cc=oc)).wait_recv()
            compute(args[0])
        elif op == "proj":
            project(*args)
        elif op == "sum":
            step(me, *args)

    def sent(ref, sem):
        rcopy(ref, ref, sem.at[0], rc_r.at[0, 0], dev(cc=oc)).wait_send()

    def drain(me):
        sent(upg.at[:, pl.ds(0, (Z - 1) * Dl)], wz_s)
        sent(upg.at[0], wx_s)
        sent(upg.at[0], wy_s)
        sent(upg.at[0], wd_s)
        sent(tokg.at[0, pl.ds(0, T)] if me == 0 else upg.at[:, pl.ds(0, 5 * Dl)], t_s)
        sent(tokg.at[pl.ds(0, 2)], tc_s)
        sent(zout.at[pl.ds(0, Z - 1)], rz_s)
        sent(zout, rc_s)

    for me in range(Z // 2):
        @pl.when(p == me)
        def _(me=me):
            for item in PROGRAM[me]:
                run(me, *item)
            drain(me)


def solution(mesh):
    n_fs, n_tp = mesh.shape["fs"], mesh.shape["tp"]
    X = 2 ** (int(math.log2(n_fs)) // 2)
    Z = n_fs // X
    C = 2
    Y = n_tp // C
    placed = (P(("fs", "tp"), None), P(), P("fs", "tp"), P("tp", "fs"))

    def on_device(tokens, norm_gain, up_weight, down_weight):
        T, D = tokens.shape
        Dl, FFl = up_weight.shape
        B = FFl // Z
        if X != 2 or Y != 2 or Z != 4 or Z * X != n_fs or Dl % 256 or B % 256 or T % (16 * CUTS):
            return plain(tokens, norm_gain, up_weight, down_weight)
        F = Z * X
        dma = pltpu.SemaphoreType.DMA
        vm = pl.BlockSpec(memory_space=pltpu.VMEM)
        hbm = pl.BlockSpec(memory_space=pltpu.HBM)
        return pl.pallas_call(
            functools.partial(kernel, Z, X, Y, C),
            out_shape=jax.ShapeDtypeStruct((T, D), bf16),
            in_specs=[hbm] * 4,
            out_specs=vm,
            scratch_shapes=[
                pltpu.VMEM((T, D), bf16),
                pltpu.VMEM((1, D), f32),
                pltpu.VMEM((Dl, FFl), bf16),
                pltpu.VMEM((FFl, Dl), bf16),
                pltpu.VMEM((Z, C * T, D), bf16),
                pltpu.VMEM((Y, D, B), bf16),
                pltpu.VMEM((Z, Y * B, X * Dl), bf16),
                pltpu.VMEM((Z, C * T, Y * B), bf16),
                pltpu.VMEM((Z, F, C, T, Dl), bf16),
                pltpu.VMEM((Z, F, T, Dl), bf16),
                pltpu.VMEM((Z + 1, F, T, Dl), bf16),
                pltpu.VMEM((Z, F, T, Dl), bf16),
                dma((6,)),
                *[dma((1,)) for _ in range(8)],
                dma((2, Z, 2)), dma((2, Z)), dma((2, Z)), dma((2, Z)),
                dma((Z, CUTS)), dma((Z,)), dma((Z, Z)), dma((Z + 1, F)),
            ],
            compiler_params=pltpu.CompilerParams(
                collective_id=0, has_side_effects=True, vmem_limit_bytes=48 * 2**20),
        )(*[pltpu.with_memory_space_constraint(v, pltpu.HBM)
            for v in (tokens, norm_gain.reshape(1, D), up_weight, down_weight)])

    return jax.shard_map(
        on_device, mesh=mesh, in_specs=placed, out_specs=P(("fs", "tp"), None), check_vma=False)
```
